32 devices in a mesh: sp: 8 (over z, y), dp: 4 (over x, core).
Axes of the slice: x: 2, y: 2, z: 4, core: 2. Of those that a mesh axis runs over, the one named last changes fastest.
Arguments:
- cotangent: bfloat16 [4, 2048, 4096], P('dp', 'sp'), may hold values from -6 to 6
- up_pre: bfloat16 [4, 2048, 4096], P('dp', 'sp'), may hold values from -6 to 6
- value_pre: bfloat16 [4, 2048, 4096], P('dp', 'sp'), may hold values from -6 to 6
- spatial_weight: bfloat16 [32, 1024, 1024], P('sp', 'dp'), may hold values from -0.1875 to 0.1875
- spatial_bias: float32 [32, 1024], P('sp'), may hold values from 0.5 to 1.5
- value_gain: float32 [4096], replicated, may hold values from 0.1 to 1.9
Outputs:
- up_grad: bfloat16 [4, 2048, 4096], P('dp', 'sp')
- value_grad: bfloat16 [4, 2048, 4096], P('dp', 'sp')
- weight_grad: float32 [32, 1024, 1024], P('sp', 'dp')
- bias_grad: float32 [32, 1024], P('sp', 'dp')
- gain_grad: float32 [4096], replicated
The draws below stay inside these ranges and needn't reach their ends.
All inputs are finite; a program needn't handle non-finite values.
Results may differ from the reference program's by a relative error of at most 0.0064.
Values may be sent and summed in bfloat16 or wider, within the bound.
A program may use at most 128 MiB of HBM per device.

```python
import math
import jax
import jax.numpy as jnp
from jax import lax

GROUPS = 32
GROUP = 128
BLOCK = 1024
WIDTH = 4096
SEQ = 2048
BATCH = 4


def shard_levels(key, shape, pieces, least, high):
    gain = 1.0
    for axis_at, parts in pieces:
        draws = jax.random.uniform(jax.random.fold_in(jax.random.fold_in(key, 6), axis_at), (parts,), jnp.float32, least / len(pieces), high / len(pieces))
        gain = gain * jnp.repeat(jnp.exp(draws), shape[axis_at] // parts).reshape((-1,) + (1,) * (len(shape) - 1 - axis_at))
    return gain


def centred(rng, dims, spread, most, pieces=(), dtype=jnp.bfloat16):
    values = jax.random.normal(rng, dims, jnp.float32) * spread
    if len(pieces) > 0:
        values = shard_levels(rng, dims, pieces, -0.22, 0.18) * values
    return jnp.clip(values, min=-most, max=most).astype(dtype)


def setup_inputs(seed: int = 0) -> dict:
    streams_of = jax.random.split(jax.random.key(seed), 7)
    return {
        "cotangent": centred(streams_of[0], (BATCH, SEQ, WIDTH), 1.0, 6.0, ((0, 4), (1, 8))),
        "up_pre": centred(streams_of[1], (BATCH, SEQ, WIDTH), 1.0, 6.0, ((0, 4), (1, 8))),
        "value_pre": centred(streams_of[2], (BATCH, SEQ, WIDTH), 1.0, 6.0, ((0, 4), (1, 8))),
        "spatial_weight": centred(streams_of[3], (GROUPS, BLOCK, BLOCK), BLOCK ** -0.5, 0.1875, ((0, 8), (1, 4))),
        "spatial_bias": jnp.clip(0.5 + 1.0 * jax.random.uniform(streams_of[4], (GROUPS, BLOCK), jnp.float32) ** shard_levels(streams_of[4], (GROUPS, BLOCK), ((0, 8),), -0.2, 0.2), 0.5, 1.5),
        "value_gain": jnp.clip(1.0 + 0.18 * jax.random.normal(streams_of[5], (WIDTH,), jnp.float32), 0.1, 1.9),
    }


norm_floor = 0.5
root_half = 1.0 / math.sqrt(2.0)
inv_root_tau = 1.0 / math.sqrt(2.0 * math.pi)

def gelu_slope(values):
    return 0.5 * (1.0 + jax.scipy.special.erf(values * root_half)) + values * jnp.exp(-0.5 * values * values) * inv_root_tau

def reference(cotangent, up_pre, value_pre, spatial_weight, spatial_bias, value_gain):
    weight_full = spatial_weight.astype(jnp.float32)
    bias_full = spatial_bias.astype(jnp.float32).T[None, :, :, None]
    gain_full = value_gain.astype(jnp.float32)
    block_shape = (SEQ // BLOCK, BLOCK, GROUPS, GROUP)

    def one_sequence(carried, inputs):
        grad_seq, up_seq, value_seq = inputs
        grad_tok = grad_seq.astype(jnp.float32)
        up_arg = up_seq.astype(jnp.float32)
        value_arg = value_seq.astype(jnp.float32)
        up_act = lax.optimization_barrier(jax.nn.gelu(up_arg, approximate=False).astype(jnp.bfloat16))
        value_act = jax.nn.gelu(value_arg, approximate=False)
        inv_rms = lax.rsqrt(lax.optimization_barrier(jnp.mean(value_act * value_act, axis=-1, keepdims=True)) + norm_floor)
        normed = value_act * inv_rms
        value_norm = lax.optimization_barrier((normed * gain_full).astype(jnp.bfloat16))
        gate_tok = lax.optimization_barrier((grad_tok * up_act.astype(jnp.float32)).astype(jnp.bfloat16))
        value_blocks = value_norm.astype(jnp.float32).reshape(block_shape)
        gate_blocks = gate_tok.astype(jnp.float32).reshape(block_shape)
        mixed_out = jnp.einsum('gpq,nqgc->npgc', weight_full, value_blocks) + bias_full
        mixed_out = lax.optimization_barrier(mixed_out.astype(jnp.bfloat16).reshape(SEQ, WIDTH))
        back_seq = jnp.einsum('gpq,npgc->nqgc', weight_full, gate_blocks)
        back_seq = lax.optimization_barrier(back_seq.astype(jnp.bfloat16).reshape(SEQ, WIDTH))
        weight_acc = carried[0] + jnp.einsum('npgc,nqgc->gpq', gate_blocks, value_blocks)
        bias_acc = carried[1] + lax.optimization_barrier(jnp.sum(gate_blocks, axis=(0, 3))).T
        up_mid = lax.optimization_barrier((grad_tok * mixed_out.astype(jnp.float32)).astype(jnp.bfloat16))
        up_out = (up_mid.astype(jnp.float32) * gelu_slope(up_arg)).astype(jnp.bfloat16)
        back_full = back_seq.astype(jnp.float32)
        gain_acc = carried[2] + lax.optimization_barrier(jnp.sum(back_full * normed, axis=0))
        scaled = back_full * gain_full
        value_slope = inv_rms * scaled - inv_rms ** 3 * value_act * lax.optimization_barrier(jnp.mean(scaled * value_act, axis=-1, keepdims=True))
        value_out = (value_slope * gelu_slope(value_arg)).astype(jnp.bfloat16)
        return ((weight_acc, bias_acc, gain_acc), (up_out, value_out))
    initial = (jnp.zeros((GROUPS, BLOCK, BLOCK), jnp.float32), jnp.zeros((GROUPS, BLOCK), jnp.float32), jnp.zeros((WIDTH,), jnp.float32))
    totals, outputs = lax.scan(one_sequence, initial, (cotangent, up_pre, value_pre))
    return (outputs[0], outputs[1], totals[0], totals[1], totals[2])
```

```python
import functools
import math

import jax
import jax.numpy as jnp
from jax import lax
from jax.experimental import pallas as pl
from jax.experimental.pallas import tpu as pltpu
from jax.sharding import PartitionSpec as P

norm_floor = 0.5
root_half = 1.0 / math.sqrt(2.0)
inv_root_tau = 1.0 / math.sqrt(2.0 * math.pi)
MESH = pl.DeviceIdType.MESH
f32 = jnp.float32
bf16 = jnp.bfloat16


def phi(x):
    return 0.5 + 0.5 * lax.erf(x * root_half)


def slope(x):
    return phi(x) + x * jnp.exp(-0.5 * x * x) * inv_root_tau


def drain(ref, sem):
    pltpu.make_async_copy(ref, ref, sem).wait()


def loop(count, body):
    def step(i, carry):
        body(i)
        return carry

    lax.fori_loop(0, count, step, 0)


def kernel(
    S, D, gd, tok, block, blocks, c,
    cot, up, val, w, bias_in, gain_in,
    up_o, val_o, wg_o, bg_o, gg_o,
    cot_v, up_v, val_v, gate_s, norm_s, gate_h, norm_h, w_full, back_s, mix_s, back_t, mix_t,
    wg_s, wg_r, act, inv_b, bias_s, bias_r, gain_all, gain_d, bias, gain,
    in_ab, in_v, in_w, in_p, w_snd, w_rx, w_rc, w_rr, w_fwd,
    g_snd, g_rcv, v_snd, v_rcv, b_snd, b_rcv, m_snd, m_rcv, wg_snd, wg_rcv,
    bs_snd, bs_rcv, gn_snd, gn_rcv, gx_snd, gx_rcv,
):
    s = lax.axis_index("sp")
    d = lax.axis_index("dp")
    groups = S * gd
    rows = block // D
    per_block = block // tok
    half = D // 2
    twin = d + 1 - 2 * lax.rem(d, 2)
    width = groups * c

    def lanes(i, n):
        return pl.ds(pl.multiple_of(i * n, 128), n)

    def sub(i, n):
        return pl.ds(pl.multiple_of(i * n, n), n)

    my_rows = sub(lax.rem(s, per_block), tok)
    my_cols = lanes(s // per_block, c)

    mid = S // 2

    def order(k):
        far = mid - mid * (s // mid) + lax.rem(s + k, mid)
        near = mid * (s // mid) + lax.rem(s + k + 1 - mid, mid)
        return jnp.where(k < mid, far, near)

    def remote(src, dst, snd, rcv, sp, dp):
        pltpu.make_async_remote_copy(
            src_ref=src, dst_ref=dst, send_sem=snd, recv_sem=rcv,
            device_id=(sp, dp), device_id_type=MESH,
        ).start()

    def fetch(g):
        def one(j):
            n = j * gd + g
            pltpu.make_async_copy(up.at[0, :, lanes(n, c)], up_v.at[n], in_ab.at[g, 0]).start()
            pltpu.make_async_copy(cot.at[0, :, lanes(n, c)], cot_v.at[n], in_ab.at[g, 1]).start()
        loop(S, one)

    barrier = pltpu.get_barrier_semaphore()
    loop(S - 1, lambda k: pl.semaphore_signal(
        barrier, inc=1, device_id=(lax.rem(s + k + 1, S), d), device_id_type=MESH))
    loop(D - 1, lambda k: pl.semaphore_signal(
        barrier, inc=1, device_id=(s, lax.rem(d + k + 1, D)), device_id_type=MESH))
    loop(gd, fetch)
    pl.semaphore_wait(barrier, S + D - 2)

    def send_weights(g):
        mine = w_full.at[g, sub(d, rows)]
        loop(half - 1, lambda k: remote(
            w.at[g], mine, w_snd, w_rx.at[g, k], s, lax.rem(d + 2 * k + 2, D)))
        remote(w.at[g], mine, w_snd, w_rc.at[g], s, twin)

    def gate_group(g):
        drain(up_v.at[pl.ds(0, S)], in_ab.at[g, 0])
        drain(cot_v.at[pl.ds(0, S)], in_ab.at[g, 1])

        def chunk(n):
            x = up_v[n].astype(f32)
            a = (x * phi(x)).astype(bf16)
            return (cot_v[n].astype(f32) * a.astype(f32)).astype(bf16)

        def one(k):
            peer = order(k)
            n = peer * gd + g
            gate_s[n] = chunk(n)
            remote(gate_s.at[n], gate_h.at[g, my_rows, my_cols], g_snd, g_rcv.at[g], peer, d)

        loop(S - 1, one)
        gate_h[g, my_rows, my_cols] = chunk(s * gd + g)

    gate_group(0)
    loop(gd, lambda g: pltpu.make_async_copy(w.at[g], w_full.at[g, sub(d, rows)], in_w.at[g]).start())
    loop(gd, send_weights)
    pltpu.make_async_copy(bias_in, bias, in_p.at[0]).start()
    pltpu.make_async_copy(gain_in, gain, in_p.at[1]).start()
    loop(groups, lambda n: pltpu.make_async_copy(val.at[0, :, lanes(n, c)], val_v.at[n], in_v).start())
    loop(gd - 1, lambda g: gate_group(g + 1))

    drain(val_v, in_v)
    drain(bias, in_p.at[0])
    drain(gain, in_p.at[1])

    def stat(n, acc):
        x = val_v[n].astype(f32)
        a = x * phi(x)
        act[n] = a
        return acc + a * a

    total = lax.fori_loop(0, groups, stat, jnp.zeros((tok, c), f32))
    mean = jnp.sum(total, axis=1, keepdims=True) / width
    inv_b[...] = jnp.broadcast_to(lax.rsqrt(mean + norm_floor), (tok, c))

    def norm_group(g):
        def chunk(n):
            return (act[n] * inv_b[...] * gain[n]).astype(bf16)

        def one(k):
            peer = order(k)
            n = peer * gd + g
            norm_s[n] = chunk(n)
            remote(norm_s.at[n], norm_h.at[g, my_rows, my_cols], v_snd, v_rcv.at[g], peer, d)

        loop(S - 1, one)
        norm_h[g, my_rows, my_cols] = chunk(s * gd + g)

    loop(gd, norm_group)

    part = block * (S - 1) // S
    tile = min(block, 256)

    def give_back(g, src, dst, snd, rcv, near):
        def one(k):
            peer = order(S - 2 - k if near else k)
            remote(
                src.at[g, sub(lax.rem(peer, per_block), tok), lanes(peer // per_block, c)],
                dst.at[s * gd + g], snd, rcv, peer, d)

        loop(S - 1, one)
        dst[s * gd + g] = src[g, my_rows, my_cols]

    def back_group(g):
        def forward(k):
            came = lax.rem(d + D - 2 * k - 2, D)
            piece = w_full.at[g, sub(came, rows)]
            drain(piece, w_rx.at[g, k])
            remote(piece, piece, w_fwd, w_rr.at[g, k], s, twin)

        loop(half - 1, forward)
        drain(w_full.at[g, pl.ds(0, rows)], w_rc.at[g])
        drain(w_full.at[g, pl.ds(0, rows)], in_w.at[g])
        loop(half - 1, lambda k: drain(w_full.at[g, pl.ds(0, rows)], w_rr.at[g, k]))
        drain(gate_h.at[g, pl.ds(0, part)], g_rcv.at[g])

        def one(t):
            cols = lanes(t, tile)
            y = lax.dot_general(
                w_full[g, :, cols], gate_h[g], (((0,), (0,)), ((), ())), preferred_element_type=f32)
            back_s[g, sub(t, tile), :] = y.astype(bf16)

        loop(block // tile, one)
        give_back(g, back_s, back_t, b_snd, b_rcv, False)
        bias_s[g] = lax.dot_general(
            jnp.ones((8, blocks * c), bf16), gate_h[g], (((1,), (1,)), ((), ())),
            preferred_element_type=f32)

    loop(gd, back_group)
    loop(D - 1, lambda k: remote(
        bias_s.at[:, :, lanes(lax.rem(d + k + 1, D), rows)], bias_r.at[k], bs_snd, bs_rcv,
        s, lax.rem(d + k + 1, D)))

    def mix_group(g):
        drain(norm_h.at[g, pl.ds(0, part)], v_rcv.at[g])
        n = s * gd + g

        def dot(t, acc):
            at = sub(t, 32)
            return acc + back_s[g, at, :].astype(f32) * norm_h[g, at, :].astype(f32)

        total = lax.fori_loop(0, block // 32, dot, jnp.zeros((32, blocks * c), f32))
        total = jnp.sum(total, axis=0, keepdims=True)
        total = sum(total[:, b * c:(b + 1) * c] for b in range(blocks))
        gain_d[g, d] = total / gain[n]
        loop(D - 1, lambda k: remote(
            gain_d.at[g, d], gain_d.at[g, d], gx_snd, gx_rcv.at[g], s, lax.rem(d + k + 1, D)))

        def grad(peer):
            return lax.dot_general(
                gate_h[g, sub(peer, rows), :], norm_h[g], (((1,), (1,)), ((), ())),
                preferred_element_type=f32)

        def one(k):
            peer = lax.rem(d + k + 1, D)
            wg_s[g, k] = grad(peer).astype(bf16)
            remote(wg_s.at[g, k], wg_r.at[g, k], wg_snd, wg_rcv.at[g], s, peer)

        loop(D - 1, one)

        def mul(t):
            at = sub(t, tile)
            y = jnp.dot(w_full[g, at, :], norm_h[g], preferred_element_type=f32)
            col = jnp.broadcast_to(bias[pl.ds(g, 1), lanes(t, tile)], (c, tile)).T
            mix_s[g, at, :] = (y + jnp.concatenate([col] * blocks, axis=1)).astype(bf16)

        loop(block // tile, mul)
        drain(gain_d.at[g, pl.ds(0, D - 1)], gx_rcv.at[g])
        gain_all[n] = lax.fori_loop(
            0, D, lambda k, acc: acc + gain_d[g, k], jnp.zeros((1, c), f32))
        loop(S - 1, lambda k: remote(
            gain_all.at[n], gain_all.at[n], gn_snd, gn_rcv, order(k), d))
        give_back(g, mix_s, mix_t, m_snd, m_rcv.at[g], True)
        wg_o[g] = grad(d)

    loop(gd, mix_group)

    drain(back_t.at[pl.ds(0, (S - 1) * gd)], b_rcv)

    def dots(n, acc):
        return acc + back_t[n].astype(f32) * act[n] * gain[n]

    total = lax.fori_loop(0, groups, dots, jnp.zeros((tok, c), f32))
    coef = jnp.sum(total, axis=1, keepdims=True) / width

    def value_out(n):
        inv = inv_b[...]
        scaled = back_t[n].astype(f32) * gain[n]
        y = inv * scaled - inv * inv * inv * act[n] * coef
        val_o[0, :, lanes(n, c)] = (y * slope(val_v[n].astype(f32))).astype(bf16)

    loop(groups, value_out)

    drain(bias_r, bs_rcv)
    total = lax.fori_loop(
        0, D - 1, lambda k, acc: acc + bias_r[k], bias_s[:, :, lanes(d, rows)])
    bg_o[...] = total[:, 0, :]

    def up_slope(n):
        act[n] = slope(up_v[n].astype(f32))

    loop(groups, up_slope)

    def sum_weight_grad(g):
        drain(wg_r.at[g], wg_rcv.at[g])

        def one(t):
            at = sub(t, 32)
            acc = wg_o[g, at, :]
            for k in range(D - 1):
                acc = acc + wg_r[g, k, at, :].astype(f32)
            wg_o[g, at, :] = acc

        loop(rows // 32, one)

    loop(gd, sum_weight_grad)

    def up_group(g):
        drain(mix_t.at[pl.ds(0, S - 1)], m_rcv.at[g])

        def one(j):
            n = j * gd + g
            mid = (cot_v[n].astype(f32) * mix_t[n].astype(f32)).astype(bf16)
            up_o[0, :, lanes(n, c)] = (mid.astype(f32) * act[n]).astype(bf16)

        loop(S, one)

    loop(gd, up_group)
    chunks = pl.ds(0, (S - 1) * gd)
    drain(gain_all.at[chunks], gn_rcv)
    gg_o[...] = gain_all[...]

    drain(w_full.at[:, pl.ds(0, half * rows)], w_snd)
    if half > 1:
        drain(w_full.at[:, pl.ds(0, (half - 1) * rows)], w_fwd)
    drain(gate_s.at[chunks], g_snd)
    drain(norm_s.at[chunks], v_snd)
    drain(back_t.at[chunks], b_snd)
    drain(mix_t.at[chunks], m_snd)
    drain(wg_s, wg_snd)
    drain(bias_r, bs_snd)
    drain(gain_d.at[:, pl.ds(0, D - 1)], gx_snd)
    drain(gain_all.at[chunks], gn_snd)


def finish(*refs):
    ins, outs, sems = refs[:5], refs[5:10], refs[10]
    copies = [pltpu.make_async_copy(a, b, sems.at[i]) for i, (a, b) in enumerate(zip(ins, outs))]
    for copy in copies:
        copy.start()
    for copy in copies:
        copy.wait()


def shards(S, D, cotangent, up_pre, value_pre, spatial_weight, spatial_bias, value_gain):
    tok, width = cotangent.shape[1:]
    gd, rows, block = spatial_weight.shape
    groups = gd * S
    c = width // groups
    blocks = tok * S // block
    half = D // 2
    dma = pltpu.SemaphoreType.DMA
    vm = pltpu.VMEM
    tokens = vm((groups, tok, c), bf16)
    heads = vm((gd, block, blocks * c), bf16)
    scratch = [
        tokens, tokens, tokens, tokens, tokens, heads, heads,
        vm((gd, block, block), bf16), heads, heads, tokens, tokens,
        vm((gd, D - 1, rows, block), bf16), vm((gd, D - 1, rows, block), bf16),
        vm((groups, tok, c), f32), vm((tok, c), f32),
        vm((gd, 8, block), f32), vm((D - 1, gd, 8, rows), f32),
        vm((groups, 1, c), f32), vm((gd, D, 1, c), f32), vm((gd, block), f32), vm((groups, 1, c), f32),
        dma((gd, 2)), dma, dma((gd,)), dma((2,)), dma, dma((gd, half)), dma((gd,)), dma((gd, half)), dma,
        dma, dma((gd,)), dma, dma((gd,)), dma, dma, dma, dma((gd,)), dma, dma((gd,)),
        dma, dma, dma, dma, dma, dma((gd,)),
    ]
    anywhere = pl.BlockSpec(memory_space=pl.ANY)
    local = pl.BlockSpec(memory_space=pltpu.VMEM)
    outs = pl.pallas_call(
        functools.partial(kernel, S, D, gd, tok, block, blocks, c),
        out_shape=(
            vm((1, tok, width), bf16), vm((1, tok, width), bf16), vm((gd, rows, block), f32),
            vm((gd, rows), f32), vm((groups, 1, c), f32),
        ),
        in_specs=[anywhere] * 6,
        out_specs=(local,) * 5,
        scratch_shapes=scratch,
        compiler_params=pltpu.CompilerParams(
            collective_id=0, has_side_effects=True, vmem_limit_bytes=55 * 2**20),
    )(
        cotangent, up_pre, value_pre, spatial_weight,
        spatial_bias, value_gain.reshape(groups, 1, c),
    )
    outs = pl.pallas_call(
        finish,
        out_shape=[jax.ShapeDtypeStruct(o.shape, o.dtype) for o in outs],
        in_specs=[anywhere] * 5,
        out_specs=[anywhere] * 5,
        scratch_shapes=[dma((5,))],
        compiler_params=pltpu.CompilerParams(vmem_limit_bytes=2**20),
    )(*outs)
    return (*outs[:4], outs[4].reshape(width))


def solution(mesh):
    tokens = P("dp", "sp", None)
    return jax.shard_map(
        functools.partial(shards, mesh.shape["sp"], mesh.shape["dp"]),
        mesh=mesh,
        in_specs=(tokens, tokens, tokens, P("sp", "dp", None), P("sp", None), P()),
        out_specs=(tokens, tokens, P("sp", "dp", None), P("sp", "dp"), P()),
        check_vma=False,
    )
```

```python
import functools
import math

import jax
import jax.numpy as jnp
from jax import lax
from jax.experimental import pallas as pl
from jax.experimental.pallas import tpu as pltpu
from jax.sharding import PartitionSpec as P

norm_floor = 0.5
root_half = 1.0 / math.sqrt(2.0)
inv_root_tau = 1.0 / math.sqrt(2.0 * math.pi)
MESH = pl.DeviceIdType.MESH
f32 = jnp.float32
bf16 = jnp.bfloat16


def phi(x):
    return 0.5 + 0.5 * lax.erf(x * root_half)


def slope(x):
    return phi(x) + x * jnp.exp(-0.5 * x * x) * inv_root_tau


def drain(ref, sem):
    pltpu.make_async_copy(ref, ref, sem).wait()


def loop(count, body):
    def step(i, carry):
        body(i)
        return carry

    lax.fori_loop(0, count, step, 0)


def kernel(
    S, D, gd, tok, block, blocks, c,
    cot, up, val, w, bias_in, gain_in,
    up_o, val_o, wg_o, bg_o, gg_o,
    cot_v, up_v, val_v, gate_s, norm_s, gate_h, norm_h, w_full, back_s, mix_s, back_t, mix_t,
    wg_s, wg_t, wg_f, wg_r, act, inv_b, bias_s, bias_r, gain_all, gain_d, bias, gain,
    in_ab, in_v, in_w, in_p, w_snd, w_rx, w_rc, w_rr, w_fwd,
    g_snd, g_rcv, v_snd, v_rcv, b_snd, b_rcv, m_snd, m_rcv, wt_snd, wt_rcv, wg_snd, wg_rcv,
    bs_snd, bs_rcv, gn_snd, gn_rcv, gx_snd, gx_rcv,
):
    s = lax.axis_index("sp")
    d = lax.axis_index("dp")
    groups = S * gd
    rows = block // D
    per_block = block // tok
    half = D // 2
    twin = d + 1 - 2 * lax.rem(d, 2)
    width = groups * c

    def lanes(i, n):
        return pl.ds(pl.multiple_of(i * n, 128), n)

    def sub(i, n):
        return pl.ds(pl.multiple_of(i * n, n), n)

    my_rows = sub(lax.rem(s, per_block), tok)
    my_cols = lanes(s // per_block, c)

    mid = S // 2
    quart = S // 4

    def order(k):
        far = mid - mid * (s // mid) + quart * (k // quart) + lax.rem(s + k, quart)
        near = mid * (s // mid) + lax.rem(s + k + 1 - mid, mid)
        return jnp.where(k < mid, far, near)

    def late_order(k):
        return order(jnp.where(k < mid - 1, k + mid, k - mid + 1))

    def remote(src, dst, snd, rcv, sp, dp):
        pltpu.make_async_remote_copy(
            src_ref=src, dst_ref=dst, send_sem=snd, recv_sem=rcv,
            device_id=(sp, dp), device_id_type=MESH,
        ).start()

    def fetch(g):
        def one(j):
            n = j * gd + g
            pltpu.make_async_copy(up.at[0, :, lanes(n, c)], up_v.at[n], in_ab.at[g, 0]).start()
            pltpu.make_async_copy(cot.at[0, :, lanes(n, c)], cot_v.at[n], in_ab.at[g, 1]).start()
        loop(S, one)

    barrier = pltpu.get_barrier_semaphore()
    loop(S - 1, lambda k: pl.semaphore_signal(
        barrier, inc=1, device_id=(lax.rem(s + k + 1, S), d), device_id_type=MESH))
    loop(D - 1, lambda k: pl.semaphore_signal(
        barrier, inc=1, device_id=(s, lax.rem(d + k + 1, D)), device_id_type=MESH))
    loop(gd, fetch)
    pl.semaphore_wait(barrier, S + D - 2)

    def send_weights(g):
        mine = w_full.at[g, sub(d, rows)]
        loop(half - 1, lambda k: remote(
            w.at[g], mine, w_snd, w_rx.at[g, k], s, lax.rem(d + 2 * k + 2, D)))
        remote(w.at[g], mine, w_snd, w_rc.at[g], s, twin)

    def gate_group(g):
        drain(up_v.at[pl.ds(0, S)], in_ab.at[g, 0])
        drain(cot_v.at[pl.ds(0, S)], in_ab.at[g, 1])

        def chunk(n):
            x = up_v[n].astype(f32)
            a = (x * phi(x)).astype(bf16)
            return (cot_v[n].astype(f32) * a.astype(f32)).astype(bf16)

        def one(k):
            peer = order(k)
            n = peer * gd + g
            gate_s[n] = chunk(n)
            remote(gate_s.at[n], gate_h.at[g, my_rows, my_cols], g_snd, g_rcv.at[g], peer, d)

        loop(S - 1, one)
        gate_h[g, my_rows, my_cols] = chunk(s * gd + g)

    gate_group(0)
    loop(gd, lambda g: pltpu.make_async_copy(w.at[g], w_full.at[g, sub(d, rows)], in_w.at[g]).start())
    loop(gd, send_weights)
    pltpu.make_async_copy(bias_in, bias, in_p.at[0]).start()
    pltpu.make_async_copy(gain_in, gain, in_p.at[1]).start()
    loop(groups, lambda n: pltpu.make_async_copy(val.at[0, :, lanes(n, c)], val_v.at[n], in_v).start())
    loop(gd - 1, lambda g: gate_group(g + 1))

    drain(val_v, in_v)
    drain(bias, in_p.at[0])
    drain(gain, in_p.at[1])

    def stat(n, acc):
        x = val_v[n].astype(f32)
        a = x * phi(x)
        act[n] = a
        return acc + a * a

    total = lax.fori_loop(0, groups, stat, jnp.zeros((tok, c), f32))
    mean = jnp.sum(total, axis=1, keepdims=True) / width
    inv_b[...] = jnp.broadcast_to(lax.rsqrt(mean + norm_floor), (tok, c))

    def norm_group(g):
        def chunk(n):
            return (act[n] * inv_b[...] * gain[n]).astype(bf16)

        def one(k):
            peer = order(k)
            n = peer * gd + g
            norm_s[n] = chunk(n)
            remote(norm_s.at[n], norm_h.at[g, my_rows, my_cols], v_snd, v_rcv.at[g], peer, d)

        loop(S - 1, one)
        norm_h[g, my_rows, my_cols] = chunk(s * gd + g)

    loop(gd, norm_group)

    part = block * (S - 1) // S
    tile = min(block, 256)

    def give_back(g, src, dst, snd, rcv, near):
        def one(k):
            peer = late_order(k) if near else order(k)
            remote(
                src.at[g, sub(lax.rem(peer, per_block), tok), lanes(peer // per_block, c)],
                dst.at[s * gd + g], snd, rcv, peer, d)

        loop(S - 1, one)
        dst[s * gd + g] = src[g, my_rows, my_cols]

    def back_group(g):
        def forward(k):
            came = lax.rem(d + D - 2 * k - 2, D)
            piece = w_full.at[g, sub(came, rows)]
            drain(piece, w_rx.at[g, k])
            remote(piece, piece, w_fwd, w_rr.at[g, k], s, twin)

        loop(half - 1, forward)
        drain(w_full.at[g, pl.ds(0, rows)], w_rc.at[g])
        drain(w_full.at[g, pl.ds(0, rows)], in_w.at[g])
        loop(half - 1, lambda k: drain(w_full.at[g, pl.ds(0, rows)], w_rr.at[g, k]))
        drain(gate_h.at[g, pl.ds(0, part)], g_rcv.at[g])

        def one(t):
            cols = lanes(t, tile)
            y = lax.dot_general(
                w_full[g, :, cols], gate_h[g], (((0,), (0,)), ((), ())), preferred_element_type=f32)
            back_s[g, sub(t, tile), :] = y.astype(bf16)

        loop(block // tile, one)
        give_back(g, back_s, back_t, b_snd, b_rcv, False)
        bias_s[g] = lax.dot_general(
            jnp.ones((8, blocks * c), bf16), gate_h[g], (((1,), (1,)), ((), ())),
            preferred_element_type=f32)

    loop(gd, back_group)
    loop(D - 1, lambda k: remote(
        bias_s.at[:, :, lanes(lax.rem(d + k + 1, D), rows)], bias_r.at[k], bs_snd, bs_rcv,
        s, lax.rem(d + k + 1, D)))

    def mix_group(g):
        drain(norm_h.at[g, pl.ds(0, part)], v_rcv.at[g])
        n = s * gd + g

        def dot(t, acc):
            at = sub(t, 32)
            return acc + back_s[g, at, :].astype(f32) * norm_h[g, at, :].astype(f32)

        total = lax.fori_loop(0, block // 32, dot, jnp.zeros((32, blocks * c), f32))
        total = jnp.sum(total, axis=0, keepdims=True)
        total = sum(total[:, b * c:(b + 1) * c] for b in range(blocks))
        gain_d[g, d] = total / gain[n]
        loop(D - 1, lambda k: remote(
            gain_d.at[g, d], gain_d.at[g, d], gx_snd, gx_rcv.at[g], s, lax.rem(d + k + 1, D)))

        def grad(peer):
            return lax.dot_general(
                gate_h[g, sub(peer, rows), :], norm_h[g], (((1,), (1,)), ((), ())),
                preferred_element_type=f32)

        def pair(k):
            wg_s[g, k] = grad(lax.rem(twin + 2 * k + 2, D)).astype(bf16)
            remote(wg_s.at[g, k], wg_t.at[g, k], wt_snd, wt_rcv.at[g], s, twin)

        loop(half, pair)

        def mul(t):
            at = sub(t, tile)
            y = jnp.dot(w_full[g, at, :], norm_h[g], preferred_element_type=f32)
            col = jnp.broadcast_to(bias[pl.ds(g, 1), lanes(t, tile)], (c, tile)).T
            mix_s[g, at, :] = (y + jnp.concatenate([col] * blocks, axis=1)).astype(bf16)

        loop(block // tile, mul)
        drain(gain_d.at[g, pl.ds(0, D - 1)], gx_rcv.at[g])
        gain_all[n] = lax.fori_loop(
            0, D, lambda k, acc: acc + gain_d[g, k], jnp.zeros((1, c), f32))
        loop(S - 1, lambda k: remote(
            gain_all.at[n], gain_all.at[n], gn_snd, gn_rcv, order(k), d))
        give_back(g, mix_s, mix_t, m_snd, m_rcv.at[n], True)
        drain(wg_t.at[g], wt_rcv.at[g])

        def across(k):
            peer = lax.rem(d + 2 * k + 2, D)
            wg_f[g, k] = (grad(peer) + wg_t[g, k].astype(f32)).astype(bf16)
            remote(wg_f.at[g, k], wg_r.at[g, k], wg_snd, wg_rcv.at[g], s, peer)

        loop(half - 1, across)
        wg_o[g] = grad(d) + wg_t[g, half - 1].astype(f32)

    loop(gd, mix_group)

    drain(back_t.at[pl.ds(0, (S - 1) * gd)], b_rcv)

    def dots(n, acc):
        return acc + back_t[n].astype(f32) * act[n] * gain[n]

    total = lax.fori_loop(0, groups, dots, jnp.zeros((tok, c), f32))
    coef = jnp.sum(total, axis=1, keepdims=True) / width

    def value_out(n):
        inv = inv_b[...]
        scaled = back_t[n].astype(f32) * gain[n]
        y = inv * scaled - inv * inv * inv * act[n] * coef
        val_o[0, :, lanes(n, c)] = (y * slope(val_v[n].astype(f32))).astype(bf16)

    loop(groups, value_out)

    drain(bias_r, bs_rcv)
    total = lax.fori_loop(
        0, D - 1, lambda k, acc: acc + bias_r[k], bias_s[:, :, lanes(d, rows)])
    bg_o[...] = total[:, 0, :]

    def up_slope(n):
        act[n] = slope(up_v[n].astype(f32))

    loop(groups, up_slope)

    def sum_weight_grad(g):
        if half > 1:
            drain(wg_r.at[g], wg_rcv.at[g])

        def one(t):
            at = sub(t, 32)
            acc = wg_o[g, at, :]
            for k in range(half - 1):
                acc = acc + wg_r[g, k, at, :].astype(f32)
            wg_o[g, at, :] = acc

        loop(rows // 32, one)

    loop(gd, sum_weight_grad)

    def up_group(g):
        def chunk(n):
            mid = (cot_v[n].astype(f32) * mix_t[n].astype(f32)).astype(bf16)
            up_o[0, :, lanes(n, c)] = (mid.astype(f32) * act[n]).astype(bf16)

        def one(k):
            n = order(S - 2 - k) * gd + g
            drain(mix_t.at[n], m_rcv.at[n])
            chunk(n)

        chunk(s * gd + g)
        loop(S - 1, one)

    loop(gd, up_group)
    chunks = pl.ds(0, (S - 1) * gd)
    drain(gain_all.at[chunks], gn_rcv)
    gg_o[...] = gain_all[...]

    drain(w_full.at[:, pl.ds(0, half * rows)], w_snd)
    if half > 1:
        drain(w_full.at[:, pl.ds(0, (half - 1) * rows)], w_fwd)
    drain(gate_s.at[chunks], g_snd)
    drain(norm_s.at[chunks], v_snd)
    drain(back_t.at[chunks], b_snd)
    drain(mix_t.at[chunks], m_snd)
    drain(wg_s, wt_snd)
    if half > 1:
        drain(wg_f, wg_snd)
    drain(bias_r, bs_snd)
    drain(gain_d.at[:, pl.ds(0, D - 1)], gx_snd)
    drain(gain_all.at[chunks], gn_snd)


def finish(*refs):
    ins, outs, sems = refs[:5], refs[5:10], refs[10]
    pairs = []
    for a, b in zip(ins, outs):
        parts = min(a.shape[-2], 128) // 32 if a.ndim == 3 else 1
        size = a.shape[-2] // max(parts, 1)
        for i in range(max(parts, 1)):
            at = (slice(None), pl.ds(i * size, size)) if parts > 1 else slice(None)
            pairs.append((a.at[at], b.at[at]))
    copies = [pltpu.make_async_copy(a, b, sems.at[i]) for i, (a, b) in enumerate(pairs)]
    for copy in copies:
        copy.start()
    for copy in copies:
        copy.wait()


def shards(S, D, cotangent, up_pre, value_pre, spatial_weight, spatial_bias, value_gain):
    tok, width = cotangent.shape[1:]
    gd, rows, block = spatial_weight.shape
    groups = gd * S
    c = width // groups
    blocks = tok * S // block
    half = D // 2
    dma = pltpu.SemaphoreType.DMA
    vm = pltpu.VMEM
    tokens = vm((groups, tok, c), bf16)
    heads = vm((gd, block, blocks * c), bf16)
    scratch = [
        tokens, tokens, tokens, tokens, tokens, heads, heads,
        vm((gd, block, block), bf16), heads, heads, tokens, tokens,
        vm((gd, half, rows, block), bf16), vm((gd, half, rows, block), bf16),
        vm((gd, max(half - 1, 1), rows, block), bf16), vm((gd, max(half - 1, 1), rows, block), bf16),
        vm((groups, tok, c), f32), vm((tok, c), f32),
        vm((gd, 8, block), f32), vm((D - 1, gd, 8, rows), f32),
        vm((groups, 1, c), f32), vm((gd, D, 1, c), f32), vm((gd, block), f32), vm((groups, 1, c), f32),
        dma((gd, 2)), dma, dma((gd,)), dma((2,)), dma, dma((gd, half)), dma((gd,)), dma((gd, half)), dma,
        dma, dma((gd,)), dma, dma((gd,)), dma, dma, dma, dma((groups,)), dma, dma((gd,)), dma, dma((gd,)),
        dma, dma, dma, dma, dma, dma((gd,)),
    ]
    anywhere = pl.BlockSpec(memory_space=pl.ANY)
    local = pl.BlockSpec(memory_space=pltpu.VMEM)
    outs = pl.pallas_call(
        functools.partial(kernel, S, D, gd, tok, block, blocks, c),
        out_shape=(
            vm((1, tok, width), bf16), vm((1, tok, width), bf16), vm((gd, rows, block), f32),
            vm((gd, rows), f32), vm((groups, 1, c), f32),
        ),
        in_specs=[anywhere] * 6,
        out_specs=(local,) * 5,
        scratch_shapes=scratch,
        compiler_params=pltpu.CompilerParams(
            collective_id=0, has_side_effects=True, vmem_limit_bytes=55 * 2**20),
    )(
        cotangent, up_pre, value_pre, spatial_weight,
        spatial_bias, value_gain.reshape(groups, 1, c),
    )
    outs = pl.pallas_call(
        finish,
        out_shape=[jax.ShapeDtypeStruct(o.shape, o.dtype) for o in outs],
        in_specs=[anywhere] * 5,
        out_specs=[anywhere] * 5,
        scratch_shapes=[dma((16,))],
        compiler_params=pltpu.CompilerParams(vmem_limit_bytes=2**20),
    )(*outs)
    return (*outs[:4], outs[4].reshape(width))


def solution(mesh):
    tokens = P("dp", "sp", None)
    return jax.shard_map(
        functools.partial(shards, mesh.shape["sp"], mesh.shape["dp"]),
        mesh=mesh,
        in_specs=(tokens, tokens, tokens, P("sp", "dp", None), P("sp", None), P()),
        out_specs=(tokens, tokens, P("sp", "dp", None), P("sp", "dp"), P()),
        check_vma=False,
    )
```

```python
import functools
import math

import jax
import jax.numpy as jnp
from jax import lax
from jax.experimental import pallas as pl
from jax.experimental.pallas import tpu as pltpu
from jax.sharding import PartitionSpec as P

norm_floor = 0.5
root_half = 1.0 / math.sqrt(2.0)
inv_root_tau = 1.0 / math.sqrt(2.0 * math.pi)
MESH = pl.DeviceIdType.MESH
f32 = jnp.float32
bf16 = jnp.bfloat16


def phi(x):
    return 0.5 + 0.5 * lax.erf(x * root_half)


def slope(x):
    return phi(x) + x * jnp.exp(-0.5 * x * x) * inv_root_tau


def drain(ref, sem):
    pltpu.make_async_copy(ref, ref, sem).wait()


def loop(count, body):
    def step(i, carry):
        body(i)
        return carry

    lax.fori_loop(0, count, step, 0)


def kernel(
    S, D, gd, tok, block, blocks, c,
    cot, up, val, w, bias_in, gain_in,
    up_o, val_o, wg_o, bg_o, gg_o,
    cot_v, up_v, val_v, gate_s, norm_s, gate_h, norm_h, w_full, back_s, mix_s, back_t, mix_t,
    wg_s, wg_t, wg_f, wg_r, act, inv_b, bias_s, bias_r, gain_all, gain_d, bias, gain,
    in_ab, in_v, w_in, w_rx, sent, g_rcv, v_rcv, b_rcv, m_rcv, wt_rcv, wg_rcv, bs_rcv, gn_rcv, gx_rcv,
    last_in, near_in,
):
    s = lax.axis_index("sp")
    d = lax.axis_index("dp")
    groups = S * gd
    rows = block // D
    per_block = block // tok
    half = D // 2
    twin = d + 1 - 2 * lax.rem(d, 2)
    width = groups * c

    def lanes(i, n):
        return pl.ds(pl.multiple_of(i * n, 128), n)

    def sub(i, n):
        return pl.ds(pl.multiple_of(i * n, n), n)

    my_rows = sub(lax.rem(s, per_block), tok)
    my_cols = lanes(s // per_block, c)

    mid = S // 2
    quart = S // 4

    def order(k):
        far = mid - mid * (s // mid) + quart * (k // quart) + lax.rem(s + k, quart)
        near = mid * (s // mid) + lax.rem(s + k + 1 - mid, mid)
        return jnp.where(k < mid, far, near)

    def late_order(k):
        return order(jnp.where(k < mid - 1, k + mid, k - mid + 1))

    def remote(src, dst, snd, rcv, sp, dp):
        pltpu.make_async_remote_copy(
            src_ref=src, dst_ref=dst, send_sem=snd, recv_sem=rcv,
            device_id=(sp, dp), device_id_type=MESH,
        ).start()

    def fetch(g):
        def one(j):
            n = j * gd + g
            pltpu.make_async_copy(up.at[0, :, lanes(n, c)], up_v.at[n], in_ab.at[g]).start()
            pltpu.make_async_copy(cot.at[0, :, lanes(n, c)], cot_v.at[n], in_ab.at[g]).start()
        loop(S, one)

    barrier = pltpu.get_barrier_semaphore()
    low = s < mid

    def signal(sem, sp, dp):
        pl.semaphore_signal(sem, inc=1, device_id=(sp, dp), device_id_type=MESH)

    @pl.when(s < S - quart)
    def _():
        loop(mid, lambda k: signal(barrier, mid - mid * (s // mid) + k, d))

    loop(D - 1, lambda k: signal(barrier, s, lax.rem(d + k + 1, D)))
    loop(gd, fetch)
    pl.semaphore_wait(barrier, jnp.where(low, quart, mid) + D - 1)

    @pl.when(s >= S - quart)
    def _():
        loop(mid, lambda k: signal(last_in, k, d))

    @pl.when(s >= mid)
    def _():
        signal(near_in, s - mid, d)

    def send_weights(g):
        mine = w_full.at[g, sub(d, rows)]
        loop(half - 1, lambda k: remote(
            w.at[g], mine, sent.at[1], w_rx.at[g], s, lax.rem(d + 2 * k + 2, D)))
        remote(w.at[g], mine, sent.at[1], w_in.at[g], s, twin)

    def gate_load(g):
        drain(up_v.at[pl.ds(0, S)], in_ab.at[g])
        drain(cot_v.at[pl.ds(0, S)], in_ab.at[g])

    def gate_chunk(n):
        x = up_v[n].astype(f32)
        a = (x * phi(x)).astype(bf16)
        return (cot_v[n].astype(f32) * a.astype(f32)).astype(bf16)

    def gate_send(g, k):
        peer = order(k)
        n = peer * gd + g
        gate_s[n] = gate_chunk(n)
        remote(gate_s.at[n], gate_h.at[g, my_rows, my_cols], sent.at[0], g_rcv.at[g], peer, d)

    def gate_far(g):
        gate_load(g)
        loop(mid, lambda k: gate_send(g, k))

    def gate_near(g):
        loop(mid - 1, lambda k: gate_send(g, k + mid))
        gate_h[g, my_rows, my_cols] = gate_chunk(s * gd + g)

    gate_load(0)
    loop(quart, lambda k: gate_send(0, k))

    @pl.when(low)
    def _():
        pl.semaphore_wait(last_in, quart)
        signal(near_in, s + mid, d)

    loop(mid - quart, lambda k: gate_send(0, k + quart))
    loop(gd, lambda g: pltpu.make_async_copy(w.at[g], w_full.at[g, sub(d, rows)], w_in.at[g]).start())
    loop(gd, send_weights)
    pltpu.make_async_copy(bias_in, bias, in_v).start()
    pltpu.make_async_copy(gain_in, gain, in_v).start()
    loop(groups, lambda n: pltpu.make_async_copy(val.at[0, :, lanes(n, c)], val_v.at[n], in_v).start())
    loop(gd - 1, lambda g: gate_far(g + 1))
    pl.semaphore_wait(near_in, 1)
    loop(gd, gate_near)

    drain(val_v, in_v)
    drain(bias, in_v)
    drain(gain, in_v)

    def stat(n, acc):
        x = val_v[n].astype(f32)
        a = x * phi(x)
        act[n] = a
        return acc + a * a

    total = lax.fori_loop(0, groups, stat, jnp.zeros((tok, c), f32))
    mean = jnp.sum(total, axis=1, keepdims=True) / width
    inv_b[...] = jnp.broadcast_to(lax.rsqrt(mean + norm_floor), (tok, c))

    def norm_group(g):
        def chunk(n):
            return (act[n] * inv_b[...] * gain[n]).astype(bf16)

        def one(k):
            peer = order(k)
            n = peer * gd + g
            norm_s[n] = chunk(n)
            remote(norm_s.at[n], norm_h.at[g, my_rows, my_cols], sent.at[0], v_rcv.at[g], peer, d)

        loop(S - 1, one)
        norm_h[g, my_rows, my_cols] = chunk(s * gd + g)

    loop(gd, norm_group)

    part = block * (S - 1) // S
    tile = min(block, 256)

    def give_back(g, src, dst, snd, rcv, near):
        def one(k):
            peer = late_order(k) if near else order(k)
            remote(
                src.at[g, sub(lax.rem(peer, per_block), tok), lanes(peer // per_block, c)],
                dst.at[s * gd + g], snd, rcv, peer, d)

        loop(S - 1, one)
        dst[s * gd + g] = src[g, my_rows, my_cols]

    def back_group(g):
        def forward(k):
            piece = w_full.at[g, sub(lax.rem(d + D - 2 * k - 2, D), rows)]
            remote(piece, piece, sent.at[1], w_in.at[g], s, twin)

        if half > 1:
            drain(w_full.at[g, pl.ds(0, (half - 1) * rows)], w_rx.at[g])
            loop(half - 1, forward)
        drain(w_full.at[g, pl.ds(0, (half + 1) * rows)], w_in.at[g])
        drain(gate_h.at[g, pl.ds(0, part)], g_rcv.at[g])

        def one(t):
            cols = lanes(t, tile)
            y = lax.dot_general(
                w_full[g, :, cols], gate_h[g], (((0,), (0,)), ((), ())), preferred_element_type=f32)
            back_s[g, sub(t, tile), :] = y.astype(bf16)

        loop(block // tile, one)
        give_back(g, back_s, back_t, sent.at[0], b_rcv, False)
        bias_s[g] = lax.dot_general(
            jnp.ones((8, blocks * c), bf16), gate_h[g], (((1,), (1,)), ((), ())),
            preferred_element_type=f32)

    loop(gd, back_group)
    loop(D - 1, lambda k: remote(
        bias_s.at[:, :, lanes(lax.rem(d + k + 1, D), rows)], bias_r.at[k], sent.at[3], bs_rcv,
        s, lax.rem(d + k + 1, D)))

    def mix_group(g):
        drain(norm_h.at[g, pl.ds(0, part)], v_rcv.at[g])
        n = s * gd + g

        def dot(t, acc):
            at = sub(t, 32)
            return acc + back_s[g, at, :].astype(f32) * norm_h[g, at, :].astype(f32)

        total = lax.fori_loop(0, block // 32, dot, jnp.zeros((32, blocks * c), f32))
        total = jnp.sum(total, axis=0, keepdims=True)
        total = sum(total[:, b * c:(b + 1) * c] for b in range(blocks))
        gain_d[g, d] = total / gain[n]
        loop(D - 1, lambda k: remote(
            gain_d.at[g, d], gain_d.at[g, d], sent.at[3], gx_rcv.at[g], s, lax.rem(d + k + 1, D)))

        def grad(peer):
            return lax.dot_general(
                gate_h[g, sub(peer, rows), :], norm_h[g], (((1,), (1,)), ((), ())),
                preferred_element_type=f32)

        def pair(k):
            wg_s[g, k] = grad(lax.rem(twin + 2 * k + 2, D)).astype(bf16)
            remote(wg_s.at[g, k], wg_t.at[g, k], sent.at[2], wt_rcv.at[g], s, twin)

        loop(half, pair)

        def mul(t):
            at = sub(t, tile)
            y = jnp.dot(w_full[g, at, :], norm_h[g], preferred_element_type=f32)
            col = jnp.broadcast_to(bias[pl.ds(g, 1), lanes(t, tile)], (c, tile)).T
            mix_s[g, at, :] = (y + jnp.concatenate([col] * blocks, axis=1)).astype(bf16)

        loop(block // tile, mul)
        drain(gain_d.at[g, pl.ds(0, D - 1)], gx_rcv.at[g])
        gain_all[n] = lax.fori_loop(
            0, D, lambda k, acc: acc + gain_d[g, k], jnp.zeros((1, c), f32))
        loop(S - 1, lambda k: remote(
            gain_all.at[n], gain_all.at[n], sent.at[3], gn_rcv, order(k), d))
        give_back(g, mix_s, mix_t, sent.at[0], m_rcv.at[g], True)
        drain(wg_t.at[g], wt_rcv.at[g])

        def across(k):
            peer = lax.rem(d + 2 * k + 2, D)
            wg_f[g, k] = (grad(peer) + wg_t[g, k].astype(f32)).astype(bf16)
            remote(wg_f.at[g, k], wg_r.at[g, k], sent.at[2], wg_rcv.at[g], s, peer)

        loop(half - 1, across)
        wg_o[g] = grad(d) + wg_t[g, half - 1].astype(f32)

    loop(gd, mix_group)

    drain(back_t.at[pl.ds(0, (S - 1) * gd)], b_rcv)

    def dots(n, acc):
        return acc + back_t[n].astype(f32) * act[n] * gain[n]

    total = lax.fori_loop(0, groups, dots, jnp.zeros((tok, c), f32))
    coef = jnp.sum(total, axis=1, keepdims=True) / width

    def value_out(n):
        inv = inv_b[...]
        scaled = back_t[n].astype(f32) * gain[n]
        y = inv * scaled - inv * inv * inv * act[n] * coef
        val_o[0, :, lanes(n, c)] = (y * slope(val_v[n].astype(f32))).astype(bf16)

    loop(groups, value_out)

    drain(bias_r, bs_rcv)
    total = lax.fori_loop(
        0, D - 1, lambda k, acc: acc + bias_r[k], bias_s[:, :, lanes(d, rows)])
    bg_o[...] = total[:, 0, :]

    def up_slope(n):
        act[n] = slope(up_v[n].astype(f32))

    loop(groups, up_slope)

    def sum_weight_grad(g):
        if half > 1:
            drain(wg_r.at[g], wg_rcv.at[g])

        def one(t):
            at = sub(t, 32)
            acc = wg_o[g, at, :]
            for k in range(half - 1):
                acc = acc + wg_r[g, k, at, :].astype(f32)
            wg_o[g, at, :] = acc

        loop(rows // 32, one)

    loop(gd, sum_weight_grad)

    def up_group(g):
        def one(j):
            n = j * gd + g
            mid = (cot_v[n].astype(f32) * mix_t[n].astype(f32)).astype(bf16)
            up_o[0, :, lanes(n, c)] = (mid.astype(f32) * act[n]).astype(bf16)

        drain(mix_t.at[pl.ds(0, S - 1)], m_rcv.at[g])
        loop(S, one)

    loop(gd, up_group)
    chunks = pl.ds(0, (S - 1) * gd)
    drain(gain_all.at[chunks], gn_rcv)
    gg_o[...] = gain_all[...]

    drain(w_full.at[:, pl.ds(0, half * rows)], sent.at[1])
    if half > 1:
        drain(w_full.at[:, pl.ds(0, (half - 1) * rows)], sent.at[1])
    drain(gate_s.at[chunks], sent.at[0])
    drain(norm_s.at[chunks], sent.at[0])
    drain(back_t.at[chunks], sent.at[0])
    drain(mix_t.at[chunks], sent.at[0])
    drain(wg_s, sent.at[2])
    if half > 1:
        drain(wg_f, sent.at[2])
    drain(bias_r, sent.at[3])
    drain(gain_d.at[:, pl.ds(0, D - 1)], sent.at[3])
    drain(gain_all.at[chunks], sent.at[3])


def finish(*refs):
    ins, outs, sem = refs[:5], refs[5:10], refs[10]
    pairs = []
    for a, b in zip(ins, outs):
        parts = min(a.shape[-2], 128) // 32 if a.ndim == 3 else 1
        size = a.shape[-2] // max(parts, 1)
        for i in range(max(parts, 1)):
            at = (slice(None), pl.ds(i * size, size)) if parts > 1 else slice(None)
            pairs.append((a.at[at], b.at[at]))
    copies = [pltpu.make_async_copy(a, b, sem) for a, b in pairs]
    for copy in copies:
        copy.start()
    for copy in copies:
        copy.wait()


def shards(S, D, cotangent, up_pre, value_pre, spatial_weight, spatial_bias, value_gain):
    tok, width = cotangent.shape[1:]
    gd, rows, block = spatial_weight.shape
    groups = gd * S
    c = width // groups
    blocks = tok * S // block
    half = D // 2
    dma = pltpu.SemaphoreType.DMA
    vm = pltpu.VMEM
    tokens = vm((groups, tok, c), bf16)
    heads = vm((gd, block, blocks * c), bf16)
    scratch = [
        tokens, tokens, tokens, tokens, tokens, heads, heads,
        vm((gd, block, block), bf16), heads, heads, tokens, tokens,
        vm((gd, half, rows, block), bf16), vm((gd, half, rows, block), bf16),
        vm((gd, max(half - 1, 1), rows, block), bf16), vm((gd, max(half - 1, 1), rows, block), bf16),
        vm((groups, tok, c), f32), vm((tok, c), f32),
        vm((gd, 8, block), f32), vm((D - 1, gd, 8, rows), f32),
        vm((groups, 1, c), f32), vm((gd, D, 1, c), f32), vm((gd, block), f32), vm((groups, 1, c), f32),
        dma((gd,)), dma, dma((gd,)), dma((gd,)), dma((4,)), dma((gd,)), dma((gd,)), dma, dma((gd,)),
        dma((gd,)), dma((gd,)), dma, dma, dma((gd,)), pltpu.SemaphoreType.REGULAR, pltpu.SemaphoreType.REGULAR,
    ]
    anywhere = pl.BlockSpec(memory_space=pl.ANY)
    local = pl.BlockSpec(memory_space=pltpu.VMEM)
    outs = pl.pallas_call(
        functools.partial(kernel, S, D, gd, tok, block, blocks, c),
        out_shape=(
            vm((1, tok, width), bf16), vm((1, tok, width), bf16), vm((gd, rows, block), f32),
            vm((gd, rows), f32), vm((groups, 1, c), f32),
        ),
        in_specs=[anywhere] * 6,
        out_specs=(local,) * 5,
        scratch_shapes=scratch,
        compiler_params=pltpu.CompilerParams(
            collective_id=0, has_side_effects=True, vmem_limit_bytes=55 * 2**20),
    )(
        cotangent, up_pre, value_pre, spatial_weight,
        spatial_bias, value_gain.reshape(groups, 1, c),
    )
    outs = pl.pallas_call(
        finish,
        out_shape=[jax.ShapeDtypeStruct(o.shape, o.dtype) for o in outs],
        in_specs=[anywhere] * 5,
        out_specs=[anywhere] * 5,
        scratch_shapes=[dma],
        compiler_params=pltpu.CompilerParams(vmem_limit_bytes=2**20),
    )(*outs)
    return (*outs[:4], outs[4].reshape(width))


def solution(mesh):
    tokens = P("dp", "sp", None)
    return jax.shard_map(
        functools.partial(shards, mesh.shape["sp"], mesh.shape["dp"]),
        mesh=mesh,
        in_specs=(tokens, tokens, tokens, P("sp", "dp", None), P("sp", None), P()),
        out_specs=(tokens, tokens, P("sp", "dp", None), P("sp", "dp"), P()),
        check_vma=False,
    )
```

```python
import functools
import math

import jax
import jax.numpy as jnp
from jax import lax
from jax.experimental import pallas as pl
from jax.experimental.pallas import tpu as pltpu
from jax.sharding import PartitionSpec as P

norm_floor = 0.5
root_half = 1.0 / math.sqrt(2.0)
inv_root_tau = 1.0 / math.sqrt(2.0 * math.pi)
MESH = pl.DeviceIdType.MESH
f32 = jnp.float32
bf16 = jnp.bfloat16


def phi(x):
    return 0.5 + 0.5 * lax.erf(x * root_half)


def slope(x):
    return phi(x) + x * jnp.exp(-0.5 * x * x) * inv_root_tau


def drain(ref, sem):
    pltpu.make_async_copy(ref, ref, sem).wait()


def loop(count, body):
    def step(i, carry):
        body(i)
        return carry

    lax.fori_loop(0, count, step, 0)


def kernel(
    S, D, gd, tok, block, blocks, c,
    cot, up, val, w, bias_in, gain_in,
    up_o, val_o, wg_o, bg_o, gg_o,
    cot_v, up_v, val_v, gate_s, norm_s, gate_h, norm_h, w_full, back_s, mix_s, back_t, mix_t,
    wg_s, wg_t, wg_f, wg_r, act, inv_b, bias_s, bias_r, gain_all, gain_d, bias, gain,
    in_ab, in_v, w_in, w_rx, sent, g_rcv, v_rcv, b_rcv, m_rcv, wt_rcv, wg_rcv, bs_rcv, gn_rcv, gx_rcv,
    last_in, near_in, dp_in, in_one,
):
    s = lax.axis_index("sp")
    d = lax.axis_index("dp")
    groups = S * gd
    rows = block // D
    per_block = block // tok
    half = D // 2
    twin = d + 1 - 2 * lax.rem(d, 2)
    width = groups * c

    def lanes(i, n):
        return pl.ds(pl.multiple_of(i * n, 128), n)

    def sub(i, n):
        return pl.ds(pl.multiple_of(i * n, n), n)

    my_rows = sub(lax.rem(s, per_block), tok)
    my_cols = lanes(s // per_block, c)

    mid = S // 2
    quart = S // 4
    low = s < mid
    inner = (s >= quart) & (s < S - quart)

    def order(k):
        far = mid - mid * (s // mid) + quart * (k // quart) + lax.rem(s + k, quart)
        near = mid * (s // mid) + lax.rem(s + k + 1 - mid, mid)
        return jnp.where(k < mid, far, near)

    def late_order(k):
        return order(jnp.where(k < mid - 1, k + mid, k - mid + 1))

    def remote(src, dst, snd, rcv, sp, dp):
        pltpu.make_async_remote_copy(
            src_ref=src, dst_ref=dst, send_sem=snd, recv_sem=rcv,
            device_id=(sp, dp), device_id_type=MESH,
        ).start()

    def fetch(n, sem):
        pltpu.make_async_copy(up.at[0, :, lanes(n, c)], up_v.at[n], sem).start()
        pltpu.make_async_copy(cot.at[0, :, lanes(n, c)], cot_v.at[n], sem).start()

    def fetched(count, sem):
        drain(up_v.at[pl.ds(0, count)], sem)
        drain(cot_v.at[pl.ds(0, count)], sem)

    loop(quart, lambda k: fetch(order(k) * gd, in_one))

    barrier = pltpu.get_barrier_semaphore()

    def signal(sem, sp, dp):
        pl.semaphore_signal(sem, inc=1, device_id=(sp, dp), device_id_type=MESH)

    @pl.when(s < S - quart)
    def _():
        loop(mid, lambda k: signal(barrier, mid - mid * (s // mid) + k, d))

    loop(D - 1 - d, lambda k: signal(barrier, s, d + k + 1))
    loop(S - 1 - quart, lambda k: fetch(order(k + quart) * gd, in_ab.at[0]))
    fetch(s * gd, in_ab.at[0])
    loop(gd - 1, lambda g: loop(S, lambda j: fetch(j * gd + g + 1, in_ab.at[g + 1])))
    pl.semaphore_wait(barrier, jnp.where(low, quart, mid) + d)
    loop(d, lambda k: signal(dp_in, s, k))

    @pl.when(s >= S - quart)
    def _():
        loop(mid, lambda k: signal(last_in, k, d))

    @pl.when(s >= mid)
    def _():
        signal(near_in, s - mid, d)

    def send_weights(g):
        mine = w_full.at[g, sub(d, rows)]
        loop(half - 1, lambda k: remote(
            w.at[g], mine, sent.at[1], w_rx.at[g], s, lax.rem(d + 2 * k + 2, D)))
        remote(w.at[g], mine, sent.at[1], w_in.at[g], s, twin)

    def gate_chunk(n):
        x = up_v[n].astype(f32)
        a = (x * phi(x)).astype(bf16)
        return (cot_v[n].astype(f32) * a.astype(f32)).astype(bf16)

    def gate_send(g, k):
        peer = order(k)
        n = peer * gd + g
        gate_s[n] = gate_chunk(n)
        remote(gate_s.at[n], gate_h.at[g, my_rows, my_cols], sent.at[0], g_rcv.at[g], peer, d)

    def gate_far(g):
        fetched(S, in_ab.at[g])
        loop(mid, lambda k: gate_send(g, k))

    def gate_near(g):
        loop(mid - 1, lambda k: gate_send(g, k + mid))
        gate_h[g, my_rows, my_cols] = gate_chunk(s * gd + g)

    fetched(quart, in_one)
    loop(quart, lambda k: gate_send(0, k))

    @pl.when(low)
    def _():
        pl.semaphore_wait(last_in, quart)
        signal(near_in, s + mid, d)

    fetched(S - quart, in_ab.at[0])
    loop(mid - quart, lambda k: gate_send(0, k + quart))
    pltpu.make_async_copy(bias_in, bias, in_v).start()
    pltpu.make_async_copy(gain_in, gain, in_v).start()
    loop(groups, lambda n: pltpu.make_async_copy(val.at[0, :, lanes(n, c)], val_v.at[n], in_v).start())
    loop(gd - 1, lambda g: gate_far(g + 1))

    @pl.when(d < D - 1)
    def _():
        pl.semaphore_wait(dp_in, D - 1 - d)

    loop(gd, lambda g: pltpu.make_async_copy(w.at[g], w_full.at[g, sub(d, rows)], w_in.at[g]).start())
    loop(gd, send_weights)
    pl.semaphore_wait(near_in, 1)
    loop(gd, gate_near)

    drain(val_v, in_v)
    drain(bias, in_v)
    drain(gain, in_v)

    def stat(n, acc):
        x = val_v[n].astype(f32)
        a = x * phi(x)
        act[n] = a
        return acc + a * a

    total = lax.fori_loop(0, groups, stat, jnp.zeros((tok, c), f32))
    mean = jnp.sum(total, axis=1, keepdims=True) / width
    inv_b[...] = jnp.broadcast_to(lax.rsqrt(mean + norm_floor), (tok, c))

    def norm_group(g):
        def chunk(n):
            return (act[n] * inv_b[...] * gain[n]).astype(bf16)

        def one(k):
            peer = order(k)
            n = peer * gd + g
            norm_s[n] = chunk(n)
            remote(norm_s.at[n], norm_h.at[g, my_rows, my_cols], sent.at[0], v_rcv.at[g], peer, d)

        loop(S - 1, one)
        norm_h[g, my_rows, my_cols] = chunk(s * gd + g)

    loop(gd, norm_group)

    part = block * (S - 1) // S
    tile = min(block, 256)

    def give_back(g, src, dst, snd, rcv, near):
        def one(k):
            peer = late_order(k) if near else order(k)
            end = jnp.where((g == gd - 1) & inner & (k >= mid - 1), 1, 0) if near else 0
            remote(
                src.at[g, sub(lax.rem(peer, per_block), tok), lanes(peer // per_block, c)],
                dst.at[s * gd + g], snd, rcv.at[g + end] if near else rcv, peer, d)

        loop(S - 1, one)
        dst[s * gd + g] = src[g, my_rows, my_cols]

    def back_group(g):
        def forward(k):
            piece = w_full.at[g, sub(lax.rem(d + D - 2 * k - 2, D), rows)]
            remote(piece, piece, sent.at[1], w_in.at[g], s, twin)

        if half > 1:
            drain(w_full.at[g, pl.ds(0, (half - 1) * rows)], w_rx.at[g])
            loop(half - 1, forward)
        drain(w_full.at[g, pl.ds(0, (half + 1) * rows)], w_in.at[g])
        drain(gate_h.at[g, pl.ds(0, part)], g_rcv.at[g])

        def one(t):
            cols = lanes(t, tile)
            y = lax.dot_general(
                w_full[g, :, cols], gate_h[g], (((0,), (0,)), ((), ())), preferred_element_type=f32)
            back_s[g, sub(t, tile), :] = y.astype(bf16)

        loop(block // tile, one)
        give_back(g, back_s, back_t, sent.at[0], b_rcv, False)
        bias_s[g] = lax.dot_general(
            jnp.ones((8, blocks * c), bf16), gate_h[g], (((1,), (1,)), ((), ())),
            preferred_element_type=f32)

    loop(gd, back_group)
    loop(D - 1, lambda k: remote(
        bias_s.at[:, :, lanes(lax.rem(d + k + 1, D), rows)], bias_r.at[k], sent.at[3], bs_rcv,
        s, lax.rem(d + k + 1, D)))

    def mix_group(g):
        drain(norm_h.at[g, pl.ds(0, part)], v_rcv.at[g])
        n = s * gd + g

        def dot(t, acc):
            at = sub(t, 32)
            return acc + back_s[g, at, :].astype(f32) * norm_h[g, at, :].astype(f32)

        total = lax.fori_loop(0, block // 32, dot, jnp.zeros((32, blocks * c), f32))
        total = jnp.sum(total, axis=0, keepdims=True)
        total = sum(total[:, b * c:(b + 1) * c] for b in range(blocks))
        gain_d[g, d] = total / gain[n]
        loop(D - 1, lambda k: remote(
            gain_d.at[g, d], gain_d.at[g, d], sent.at[3], gx_rcv.at[g], s, lax.rem(d + k + 1, D)))

        def grad(peer):
            return lax.dot_general(
                gate_h[g, sub(peer, rows), :], norm_h[g], (((1,), (1,)), ((), ())),
                preferred_element_type=f32)

        def pair(k):
            wg_s[g, k] = grad(lax.rem(twin + 2 * k + 2, D)).astype(bf16)
            remote(wg_s.at[g, k], wg_t.at[g, k], sent.at[2], wt_rcv.at[g], s, twin)

        loop(half, pair)

        def mul(t):
            at = sub(t, tile)
            y = jnp.dot(w_full[g, at, :], norm_h[g], preferred_element_type=f32)
            col = jnp.broadcast_to(bias[pl.ds(g, 1), lanes(t, tile)], (c, tile)).T
            mix_s[g, at, :] = (y + jnp.concatenate([col] * blocks, axis=1)).astype(bf16)

        loop(block // tile, mul)
        drain(gain_d.at[g, pl.ds(0, D - 1)], gx_rcv.at[g])
        gain_all[n] = lax.fori_loop(
            0, D, lambda k, acc: acc + gain_d[g, k], jnp.zeros((1, c), f32))
        loop(S - 1, lambda k: remote(
            gain_all.at[n], gain_all.at[n], sent.at[3], gn_rcv, order(k), d))
        give_back(g, mix_s, mix_t, sent.at[0], m_rcv, True)
        drain(wg_t.at[g], wt_rcv.at[g])

        def across(k):
            peer = lax.rem(d + 2 * k + 2, D)
            wg_f[g, k] = (grad(peer) + wg_t[g, k].astype(f32)).astype(bf16)
            remote(wg_f.at[g, k], wg_r.at[g, k], sent.at[2], wg_rcv, s, peer)

        loop(half - 1, across)
        wg_o[g] = grad(d) + wg_t[g, half - 1].astype(f32)

    loop(gd, mix_group)

    drain(back_t.at[pl.ds(0, (S - 1) * gd)], b_rcv)

    def dots(n, acc):
        return acc + back_t[n].astype(f32) * act[n] * gain[n]

    total = lax.fori_loop(0, groups, dots, jnp.zeros((tok, c), f32))
    coef = jnp.sum(total, axis=1, keepdims=True) / width

    def value_out(n):
        inv = inv_b[...]
        scaled = back_t[n].astype(f32) * gain[n]
        y = inv * scaled - inv * inv * inv * act[n] * coef
        val_o[0, :, lanes(n, c)] = (y * slope(val_v[n].astype(f32))).astype(bf16)

    loop(groups, value_out)

    drain(bias_r, bs_rcv)
    total = lax.fori_loop(
        0, D - 1, lambda k, acc: acc + bias_r[k], bias_s[:, :, lanes(d, rows)])
    bg_o[...] = total[:, 0, :]

    def up_slope(n):
        act[n] = slope(up_v[n].astype(f32))

    loop(groups, up_slope)

    def sum_weight_grad(g):
        def one(t):
            at = sub(t, 32)
            acc = wg_o[g, at, :]
            for k in range(half - 1):
                acc = acc + wg_r[g, k, at, :].astype(f32)
            wg_o[g, at, :] = acc

        loop(rows // 32, one)

    if half > 1:
        drain(wg_r, wg_rcv)
    loop(gd, sum_weight_grad)

    def up_chunk(g, peer):
        n = peer * gd + g
        mid = (cot_v[n].astype(f32) * mix_t[n].astype(f32)).astype(bf16)
        up_o[0, :, lanes(n, c)] = (mid.astype(f32) * act[n]).astype(bf16)

    def up_group(g):
        drain(mix_t.at[pl.ds(0, S - 1)], m_rcv.at[g])
        loop(S, lambda peer: up_chunk(g, peer))

    inner_far = jnp.where(low, mid, quart)
    outer_far = jnp.where(low, mid + quart, 0)
    own = mid * (s // mid)
    loop(gd - 1, up_group)
    drain(mix_t.at[pl.ds(0, S - 1 - quart)], m_rcv.at[gd - 1])
    loop(mid, lambda k: up_chunk(gd - 1, own + k))
    loop(mid - quart, lambda k: up_chunk(gd - 1, outer_far + k))
    drain(mix_t.at[pl.ds(0, quart)], m_rcv.at[gd])
    loop(quart, lambda k: up_chunk(gd - 1, inner_far + k))
    chunks = pl.ds(0, (S - 1) * gd)
    drain(gain_all.at[chunks], gn_rcv)
    gg_o[...] = gain_all[...]

    drain(w_full.at[:, pl.ds(0, half * rows)], sent.at[1])
    if half > 1:
        drain(w_full.at[:, pl.ds(0, (half - 1) * rows)], sent.at[1])
    drain(gate_s.at[chunks], sent.at[0])
    drain(norm_s.at[chunks], sent.at[0])
    drain(back_t.at[chunks], sent.at[0])
    drain(mix_t.at[chunks], sent.at[0])
    drain(wg_s, sent.at[2])
    if half > 1:
        drain(wg_f, sent.at[2])
    drain(bias_r, sent.at[3])
    drain(gain_d.at[:, pl.ds(0, D - 1)], sent.at[3])
    drain(gain_all.at[chunks], sent.at[3])


def finish(*refs):
    ins, outs, sem = refs[:5], refs[5:10], refs[10]
    pairs = []
    for a, b in zip(ins, outs):
        parts = min(a.shape[-2], 128) // 32 if a.ndim == 3 else 1
        size = a.shape[-2] // max(parts, 1)
        for i in range(max(parts, 1)):
            at = (slice(None), pl.ds(i * size, size)) if parts > 1 else slice(None)
            pairs.append((a.at[at], b.at[at]))
    copies = [pltpu.make_async_copy(a, b, sem) for a, b in pairs]
    for copy in copies:
        copy.start()
    for copy in copies:
        copy.wait()


def shards(S, D, cotangent, up_pre, value_pre, spatial_weight, spatial_bias, value_gain):
    tok, width = cotangent.shape[1:]
    gd, rows, block = spatial_weight.shape
    groups = gd * S
    c = width // groups
    blocks = tok * S // block
    half = D // 2
    dma = pltpu.SemaphoreType.DMA
    vm = pltpu.VMEM
    tokens = vm((groups, tok, c), bf16)
    heads = vm((gd, block, blocks * c), bf16)
    scratch = [
        tokens, tokens, tokens, tokens, tokens, heads, heads,
        vm((gd, block, block), bf16), heads, heads, tokens, tokens,
        vm((gd, half, rows, block), bf16), vm((gd, half, rows, block), bf16),
        vm((gd, max(half - 1, 1), rows, block), bf16), vm((gd, max(half - 1, 1), rows, block), bf16),
        vm((groups, tok, c), f32), vm((tok, c), f32),
        vm((gd, 8, block), f32), vm((D - 1, gd, 8, rows), f32),
        vm((groups, 1, c), f32), vm((gd, D, 1, c), f32), vm((gd, block), f32), vm((groups, 1, c), f32),
        dma((gd,)), dma, dma((gd,)), dma((gd,)), dma((4,)), dma((gd,)), dma((gd,)), dma, dma((gd + 1,)),
        dma((gd,)), dma, dma, dma, dma((gd,)), pltpu.SemaphoreType.REGULAR, pltpu.SemaphoreType.REGULAR,
        pltpu.SemaphoreType.REGULAR, dma,
    ]
    anywhere = pl.BlockSpec(memory_space=pl.ANY)
    local = pl.BlockSpec(memory_space=pltpu.VMEM)
    outs = pl.pallas_call(
        functools.partial(kernel, S, D, gd, tok, block, blocks, c),
        out_shape=(
            vm((1, tok, width), bf16), vm((1, tok, width), bf16), vm((gd, rows, block), f32),
            vm((gd, rows), f32), vm((groups, 1, c), f32),
        ),
        in_specs=[anywhere] * 6,
        out_specs=(local,) * 5,
        scratch_shapes=scratch,
        compiler_params=pltpu.CompilerParams(
            collective_id=0, has_side_effects=True, vmem_limit_bytes=55 * 2**20),
    )(
        cotangent, up_pre, value_pre, spatial_weight,
        spatial_bias, value_gain.reshape(groups, 1, c),
    )
    outs = pl.pallas_call(
        finish,
        out_shape=[jax.ShapeDtypeStruct(o.shape, o.dtype) for o in outs],
        in_specs=[anywhere] * 5,
        out_specs=[anywhere] * 5,
        scratch_shapes=[dma],
        compiler_params=pltpu.CompilerParams(vmem_limit_bytes=2**20),
    )(*outs)
    return (*outs[:4], outs[4].reshape(width))


def solution(mesh):
    tokens = P("dp", "sp", None)
    return jax.shard_map(
        functools.partial(shards, mesh.shape["sp"], mesh.shape["dp"]),
        mesh=mesh,
        in_specs=(tokens, tokens, tokens, P("sp", "dp", None), P("sp", None), P()),
        out_specs=(tokens, tokens, P("sp", "dp", None), P("sp", "dp"), P()),
        check_vma=False,
    )
```

```python
import functools
import math

import jax
import jax.numpy as jnp
from jax import lax
from jax.experimental import pallas as pl
from jax.experimental.pallas import tpu as pltpu
from jax.sharding import PartitionSpec as P

norm_floor = 0.5
root_half = 1.0 / math.sqrt(2.0)
inv_root_tau = 1.0 / math.sqrt(2.0 * math.pi)
MESH = pl.DeviceIdType.MESH
f32 = jnp.float32
bf16 = jnp.bfloat16


def phi(x):
    return 0.5 + 0.5 * lax.erf(x * root_half)


def slope(x):
    return phi(x) + x * jnp.exp(-0.5 * x * x) * inv_root_tau


def drain(ref, sem):
    pltpu.make_async_copy(ref, ref, sem).wait()


def loop(count, body):
    def step(i, carry):
        body(i)
        return carry

    lax.fori_loop(0, count, step, 0)


def kernel(
    S, D, gd, tok, block, blocks, c,
    cot, up, val, w, bias_in, gain_in,
    up_o, val_o, wg_o, bg_o, gg_o,
    cot_v, up_v, val_v, gate_s, norm_s, gate_h, norm_h, w_full, back_s, mix_s, back_t, mix_t,
    wg_s, wg_t, wg_f, wg_r, act, inv_b, bias_s, bias_r, gain_all, gain_d, bias, gain,
    in_ab, in_v, w_in, w_rx, sent, g_rcv, v_rcv, b_rcv, m_rcv, wt_rcv, wg_rcv, bs_rcv, gn_rcv, gx_rcv,
    last_in, near_in, dp_in, in_one,
):
    s = lax.axis_index("sp")
    d = lax.axis_index("dp")
    groups = S * gd
    rows = block // D
    per_block = block // tok
    half = D // 2
    twin = d + 1 - 2 * lax.rem(d, 2)
    width = groups * c

    def lanes(i, n):
        return pl.ds(pl.multiple_of(i * n, 128), n)

    def sub(i, n):
        return pl.ds(pl.multiple_of(i * n, n), n)

    my_rows = sub(lax.rem(s, per_block), tok)
    my_cols = lanes(s // per_block, c)

    mid = S // 2
    quart = S // 4
    low = s < mid
    inner = (s >= quart) & (s < S - quart)

    def order(k):
        far = mid - mid * (s // mid) + quart * (k // quart) + lax.rem(s + k, quart)
        near = mid * (s // mid) + lax.rem(s + k + 1 - mid, mid)
        return jnp.where(k < mid, far, near)

    def late_order(k):
        return jnp.where(k < mid - 1, order(k + mid), mid - mid * (s // mid) + k - mid + 1)

    def remote(src, dst, snd, rcv, sp, dp):
        pltpu.make_async_remote_copy(
            src_ref=src, dst_ref=dst, send_sem=snd, recv_sem=rcv,
            device_id=(sp, dp), device_id_type=MESH,
        ).start()

    def fetch(n, sem):
        pltpu.make_async_copy(up.at[0, :, lanes(n, c)], up_v.at[n], sem).start()
        pltpu.make_async_copy(cot.at[0, :, lanes(n, c)], cot_v.at[n], sem).start()

    def fetched(count, sem):
        drain(up_v.at[pl.ds(0, count)], sem)
        drain(cot_v.at[pl.ds(0, count)], sem)

    loop(quart, lambda k: fetch(order(k) * gd, in_one))

    barrier = pltpu.get_barrier_semaphore()

    def signal(sem, sp, dp):
        pl.semaphore_signal(sem, inc=1, device_id=(sp, dp), device_id_type=MESH)

    @pl.when(s < S - quart)
    def _():
        loop(mid, lambda k: signal(barrier, mid - mid * (s // mid) + k, d))

    loop(D - 1 - d, lambda k: signal(barrier, s, d + k + 1))
    loop(S - 1 - quart, lambda k: fetch(order(k + quart) * gd, in_ab.at[0]))
    fetch(s * gd, in_ab.at[0])
    loop(gd - 1, lambda g: loop(S, lambda j: fetch(j * gd + g + 1, in_ab.at[g + 1])))
    pl.semaphore_wait(barrier, jnp.where(low, quart, mid) + d)
    loop(d, lambda k: signal(dp_in, s, k))

    @pl.when(s >= S - quart)
    def _():
        loop(mid, lambda k: signal(last_in, k, d))

    @pl.when(s >= mid)
    def _():
        signal(near_in, s - mid, d)

    def send_weights(g):
        mine = w_full.at[g, sub(d, rows)]
        loop(half - 1, lambda k: remote(
            w.at[g], mine, sent.at[1], w_rx.at[g], s, lax.rem(d + 2 * k + 2, D)))
        remote(w.at[g], mine, sent.at[1], w_in.at[g], s, twin)

    def gate_chunk(n):
        x = up_v[n].astype(f32)
        a = (x * phi(x)).astype(bf16)
        return (cot_v[n].astype(f32) * a.astype(f32)).astype(bf16)

    def gate_send(g, k):
        peer = order(k)
        n = peer * gd + g
        gate_s[n] = gate_chunk(n)
        remote(gate_s.at[n], gate_h.at[g, my_rows, my_cols], sent.at[0], g_rcv.at[g], peer, d)

    def gate_far(g):
        fetched(S, in_ab.at[g])
        loop(mid, lambda k: gate_send(g, k))

    def gate_near(g):
        loop(mid - 1, lambda k: gate_send(g, k + mid))
        gate_h[g, my_rows, my_cols] = gate_chunk(s * gd + g)

    fetched(quart, in_one)
    loop(quart, lambda k: gate_send(0, k))

    @pl.when(low)
    def _():
        pl.semaphore_wait(last_in, quart)
        signal(near_in, s + mid, d)

    fetched(S - quart, in_ab.at[0])
    loop(mid - quart, lambda k: gate_send(0, k + quart))
    pltpu.make_async_copy(bias_in, bias, in_v).start()
    pltpu.make_async_copy(gain_in, gain, in_v).start()
    loop(groups, lambda n: pltpu.make_async_copy(val.at[0, :, lanes(n, c)], val_v.at[n], in_v).start())
    loop(gd - 1, lambda g: gate_far(g + 1))

    @pl.when(d < D - 1)
    def _():
        pl.semaphore_wait(dp_in, D - 1 - d)

    loop(gd, lambda g: pltpu.make_async_copy(w.at[g], w_full.at[g, sub(d, rows)], w_in.at[g]).start())
    loop(gd, send_weights)
    pl.semaphore_wait(near_in, 1)
    loop(gd, gate_near)

    drain(val_v, in_v)
    drain(bias, in_v)
    drain(gain, in_v)

    def stat(n, acc):
        x = val_v[n].astype(f32)
        a = x * phi(x)
        act[n] = a
        return acc + a * a

    total = lax.fori_loop(0, groups, stat, jnp.zeros((tok, c), f32))
    mean = jnp.sum(total, axis=1, keepdims=True) / width
    inv_b[...] = jnp.broadcast_to(lax.rsqrt(mean + norm_floor), (tok, c))

    def norm_group(g):
        def chunk(n):
            return (act[n] * inv_b[...] * gain[n]).astype(bf16)

        def one(k):
            peer = order(k)
            n = peer * gd + g
            norm_s[n] = chunk(n)
            remote(norm_s.at[n], norm_h.at[g, my_rows, my_cols], sent.at[0], v_rcv.at[g], peer, d)

        loop(S - 1, one)
        norm_h[g, my_rows, my_cols] = chunk(s * gd + g)

    loop(gd, norm_group)

    part = block * (S - 1) // S
    tile = min(block, 256)

    def give_back(g, src, dst, snd, rcv, near):
        def one(k):
            peer = late_order(k) if near else order(k)
            end = jnp.where((g == gd - 1) & inner & (k >= mid - 1), 1, 0) if near else 0
            remote(
                src.at[g, sub(lax.rem(peer, per_block), tok), lanes(peer // per_block, c)],
                dst.at[s * gd + g], snd, rcv.at[g + end] if near else rcv, peer, d)

        loop(S - 1, one)
        dst[s * gd + g] = src[g, my_rows, my_cols]

    def back_group(g):
        def forward(k):
            piece = w_full.at[g, sub(lax.rem(d + D - 2 * k - 2, D), rows)]
            remote(piece, piece, sent.at[1], w_in.at[g], s, twin)

        if half > 1:
            drain(w_full.at[g, pl.ds(0, (half - 1) * rows)], w_rx.at[g])
            loop(half - 1, forward)
        drain(w_full.at[g, pl.ds(0, (half + 1) * rows)], w_in.at[g])
        drain(gate_h.at[g, pl.ds(0, part)], g_rcv.at[g])

        def one(t):
            cols = lanes(t, tile)
            y = lax.dot_general(
                w_full[g, :, cols], gate_h[g], (((0,), (0,)), ((), ())), preferred_element_type=f32)
            back_s[g, sub(t, tile), :] = y.astype(bf16)

        loop(block // tile, one)
        give_back(g, back_s, back_t, sent.at[0], b_rcv, False)
        bias_s[g] = lax.dot_general(
            jnp.ones((8, blocks * c), bf16), gate_h[g], (((1,), (1,)), ((), ())),
            preferred_element_type=f32)

    loop(gd, back_group)
    loop(D - 1, lambda k: remote(
        bias_s.at[:, :, lanes(lax.rem(d + k + 1, D), rows)], bias_r.at[k], sent.at[3], bs_rcv,
        s, lax.rem(d + k + 1, D)))

    def mix_group(g):
        drain(norm_h.at[g, pl.ds(0, part)], v_rcv.at[g])
        n = s * gd + g

        def dot(t, acc):
            at = sub(t, 32)
            return acc + back_s[g, at, :].astype(f32) * norm_h[g, at, :].astype(f32)

        total = lax.fori_loop(0, block // 32, dot, jnp.zeros((32, blocks * c), f32))
        total = jnp.sum(total, axis=0, keepdims=True)
        total = sum(total[:, b * c:(b + 1) * c] for b in range(blocks))
        gain_d[g, d] = total / gain[n]
        loop(D - 1, lambda k: remote(
            gain_d.at[g, d], gain_d.at[g, d], sent.at[3], gx_rcv.at[g], s, lax.rem(d + k + 1, D)))

        def grad(peer):
            return lax.dot_general(
                gate_h[g, sub(peer, rows), :], norm_h[g], (((1,), (1,)), ((), ())),
                preferred_element_type=f32)

        def pair(k):
            wg_s[g, k] = grad(lax.rem(twin + 2 * k + 2, D)).astype(bf16)
            remote(wg_s.at[g, k], wg_t.at[g, k], sent.at[2], wt_rcv.at[g], s, twin)

        loop(half, pair)

        def mul(t):
            at = sub(t, tile)
            y = jnp.dot(w_full[g, at, :], norm_h[g], preferred_element_type=f32)
            col = jnp.broadcast_to(bias[pl.ds(g, 1), lanes(t, tile)], (c, tile)).T
            mix_s[g, at, :] = (y + jnp.concatenate([col] * blocks, axis=1)).astype(bf16)

        loop(block // tile, mul)
        drain(gain_d.at[g, pl.ds(0, D - 1)], gx_rcv.at[g])
        gain_all[n] = lax.fori_loop(
            0, D, lambda k, acc: acc + gain_d[g, k], jnp.zeros((1, c), f32))
        loop(S - 1, lambda k: remote(
            gain_all.at[n], gain_all.at[n], sent.at[3], gn_rcv, order(k), d))
        give_back(g, mix_s, mix_t, sent.at[0], m_rcv, True)
        drain(wg_t.at[g], wt_rcv.at[g])

        def across(k):
            peer = lax.rem(d + 2 * k + 2, D)
            wg_f[g, k] = (grad(peer) + wg_t[g, k].astype(f32)).astype(bf16)
            remote(wg_f.at[g, k], wg_r.at[g, k], sent.at[2], wg_rcv, s, peer)

        loop(half - 1, across)
        wg_o[g] = grad(d) + wg_t[g, half - 1].astype(f32)

    loop(gd, mix_group)

    drain(back_t.at[pl.ds(0, (S - 1) * gd)], b_rcv)

    def dots(n, acc):
        return acc + back_t[n].astype(f32) * act[n] * gain[n]

    total = lax.fori_loop(0, groups, dots, jnp.zeros((tok, c), f32))
    coef = jnp.sum(total, axis=1, keepdims=True) / width

    def value_out(n):
        inv = inv_b[...]
        scaled = back_t[n].astype(f32) * gain[n]
        y = inv * scaled - inv * inv * inv * act[n] * coef
        val_o[0, :, lanes(n, c)] = (y * slope(val_v[n].astype(f32))).astype(bf16)

    loop(groups, value_out)

    drain(bias_r, bs_rcv)
    total = lax.fori_loop(
        0, D - 1, lambda k, acc: acc + bias_r[k], bias_s[:, :, lanes(d, rows)])
    bg_o[...] = total[:, 0, :]

    def up_slope(n):
        act[n] = slope(up_v[n].astype(f32))

    loop(groups, up_slope)

    def sum_weight_grad(g):
        def one(t):
            at = sub(t, 32)
            acc = wg_o[g, at, :]
            for k in range(half - 1):
                acc = acc + wg_r[g, k, at, :].astype(f32)
            wg_o[g, at, :] = acc

        loop(rows // 32, one)

    if half > 1:
        drain(wg_r, wg_rcv)
    loop(gd, sum_weight_grad)

    def up_chunk(g, peer):
        n = peer * gd + g
        mid = (cot_v[n].astype(f32) * mix_t[n].astype(f32)).astype(bf16)
        up_o[0, :, lanes(n, c)] = (mid.astype(f32) * act[n]).astype(bf16)

    def up_group(g):
        drain(mix_t.at[pl.ds(0, S - 1)], m_rcv.at[g])
        loop(S, lambda peer: up_chunk(g, peer))

    inner_far = jnp.where(low, mid, quart)
    outer_far = jnp.where(low, mid + quart, 0)
    own = mid * (s // mid)
    loop(gd - 1, up_group)
    drain(mix_t.at[pl.ds(0, S - 1 - quart)], m_rcv.at[gd - 1])
    loop(mid, lambda k: up_chunk(gd - 1, own + k))
    loop(mid - quart, lambda k: up_chunk(gd - 1, outer_far + k))
    drain(mix_t.at[pl.ds(0, quart)], m_rcv.at[gd])
    loop(quart, lambda k: up_chunk(gd - 1, inner_far + k))
    chunks = pl.ds(0, (S - 1) * gd)
    drain(gain_all.at[chunks], gn_rcv)
    gg_o[...] = gain_all[...]

    drain(w_full.at[:, pl.ds(0, half * rows)], sent.at[1])
    if half > 1:
        drain(w_full.at[:, pl.ds(0, (half - 1) * rows)], sent.at[1])
    drain(gate_s.at[chunks], sent.at[0])
    drain(norm_s.at[chunks], sent.at[0])
    drain(back_t.at[chunks], sent.at[0])
    drain(mix_t.at[chunks], sent.at[0])
    drain(wg_s, sent.at[2])
    if half > 1:
        drain(wg_f, sent.at[2])
    drain(bias_r, sent.at[3])
    drain(gain_d.at[:, pl.ds(0, D - 1)], sent.at[3])
    drain(gain_all.at[chunks], sent.at[3])


def finish(*refs):
    ins, outs, sem = refs[:5], refs[5:10], refs[10]
    pairs = []
    for a, b in zip(ins, outs):
        parts = min(a.shape[-2], 128) // 32 if a.ndim == 3 else 1
        size = a.shape[-2] // max(parts, 1)
        for i in range(max(parts, 1)):
            at = (slice(None), pl.ds(i * size, size)) if parts > 1 else slice(None)
            pairs.append((a.at[at], b.at[at]))
    copies = [pltpu.make_async_copy(a, b, sem) for a, b in pairs]
    for copy in copies:
        copy.start()
    for copy in copies:
        copy.wait()


def shards(S, D, cotangent, up_pre, value_pre, spatial_weight, spatial_bias, value_gain):
    tok, width = cotangent.shape[1:]
    gd, rows, block = spatial_weight.shape
    groups = gd * S
    c = width // groups
    blocks = tok * S // block
    half = D // 2
    dma = pltpu.SemaphoreType.DMA
    vm = pltpu.VMEM
    tokens = vm((groups, tok, c), bf16)
    heads = vm((gd, block, blocks * c), bf16)
    scratch = [
        tokens, tokens, tokens, tokens, tokens, heads, heads,
        vm((gd, block, block), bf16), heads, heads, tokens, tokens,
        vm((gd, half, rows, block), bf16), vm((gd, half, rows, block), bf16),
        vm((gd, max(half - 1, 1), rows, block), bf16), vm((gd, max(half - 1, 1), rows, block), bf16),
        vm((groups, tok, c), f32), vm((tok, c), f32),
        vm((gd, 8, block), f32), vm((D - 1, gd, 8, rows), f32),
        vm((groups, 1, c), f32), vm((gd, D, 1, c), f32), vm((gd, block), f32), vm((groups, 1, c), f32),
        dma((gd,)), dma, dma((gd,)), dma((gd,)), dma((4,)), dma((gd,)), dma((gd,)), dma, dma((gd + 1,)),
        dma((gd,)), dma, dma, dma, dma((gd,)), pltpu.SemaphoreType.REGULAR, pltpu.SemaphoreType.REGULAR,
        pltpu.SemaphoreType.REGULAR, dma,
    ]
    anywhere = pl.BlockSpec(memory_space=pl.ANY)
    local = pl.BlockSpec(memory_space=pltpu.VMEM)
    outs = pl.pallas_call(
        functools.partial(kernel, S, D, gd, tok, block, blocks, c),
        out_shape=(
            vm((1, tok, width), bf16), vm((1, tok, width), bf16), vm((gd, rows, block), f32),
            vm((gd, rows), f32), vm((groups, 1, c), f32),
        ),
        in_specs=[anywhere] * 6,
        out_specs=(local,) * 5,
        scratch_shapes=scratch,
        compiler_params=pltpu.CompilerParams(
            collective_id=0, has_side_effects=True, vmem_limit_bytes=55 * 2**20),
    )(
        cotangent, up_pre, value_pre, spatial_weight,
        spatial_bias, value_gain.reshape(groups, 1, c),
    )
    outs = pl.pallas_call(
        finish,
        out_shape=[jax.ShapeDtypeStruct(o.shape, o.dtype) for o in outs],
        in_specs=[anywhere] * 5,
        out_specs=[anywhere] * 5,
        scratch_shapes=[dma],
        compiler_params=pltpu.CompilerParams(vmem_limit_bytes=2**20),
    )(*outs)
    return (*outs[:4], outs[4].reshape(width))


def solution(mesh):
    tokens = P("dp", "sp", None)
    return jax.shard_map(
        functools.partial(shards, mesh.shape["sp"], mesh.shape["dp"]),
        mesh=mesh,
        in_specs=(tokens, tokens, tokens, P("sp", "dp", None), P("sp", None), P()),
        out_specs=(tokens, tokens, P("sp", "dp", None), P("sp", "dp"), P()),
        check_vma=False,
    )
```

```python
import functools
import math

import jax
import jax.numpy as jnp
from jax import lax
from jax.experimental import pallas as pl
from jax.experimental.pallas import tpu as pltpu
from jax.sharding import PartitionSpec as P

norm_floor = 0.5
root_half = 1.0 / math.sqrt(2.0)
inv_root_tau = 1.0 / math.sqrt(2.0 * math.pi)
MESH = pl.DeviceIdType.MESH
f32 = jnp.float32
bf16 = jnp.bfloat16


def phi(x):
    return 0.5 + 0.5 * lax.erf(x * root_half)


def slope(x):
    return phi(x) + x * jnp.exp(-0.5 * x * x) * inv_root_tau


def drain(ref, sem):
    pltpu.make_async_copy(ref, ref, sem).wait()


def loop(count, body):
    def step(i, carry):
        body(i)
        return carry

    lax.fori_loop(0, count, step, 0)


def kernel(
    S, D, gd, tok, block, blocks, c,
    cot, up, val, w, bias_in, gain_in,
    up_o, val_o, wg_o, bg_o, gg_o,
    cot_v, up_v, val_v, gate_s, norm_s, gate_h, norm_h, w_full, back_s, mix_s, back_t, mix_t,
    wg_s, wg_t, wg_f, wg_r, act, inv_b, bias_s, bias_r, gain_all, gain_d, bias, gain,
    in_ab, in_v, w_in, w_rx, sent, g_rcv, v_rcv, b_rcv, m_rcv, wt_rcv, wg_rcv, bs_rcv, gn_rcv, gx_rcv,
    last_in, near_in, dp_in, in_one,
):
    s = lax.axis_index("sp")
    d = lax.axis_index("dp")
    groups = S * gd
    rows = block // D
    per_block = block // tok
    half = D // 2
    twin = d + 1 - 2 * lax.rem(d, 2)
    width = groups * c

    def lanes(i, n):
        return pl.ds(pl.multiple_of(i * n, 128), n)

    def sub(i, n):
        return pl.ds(pl.multiple_of(i * n, n), n)

    my_rows = sub(lax.rem(s, per_block), tok)
    my_cols = lanes(s // per_block, c)

    mid = S // 2
    quart = S // 4
    low = s < mid
    inner = (s >= quart) & (s < S - quart)

    def order(k):
        far = mid - mid * (s // mid) + k
        near = mid * (s // mid) + lax.rem(s + k + 1 - mid, mid)
        return jnp.where(k < mid, far, near)

    def late_order(k):
        return order(jnp.where(k < mid - 1, k + mid, k - mid + 1))

    def remote(src, dst, snd, rcv, sp, dp):
        pltpu.make_async_remote_copy(
            src_ref=src, dst_ref=dst, send_sem=snd, recv_sem=rcv,
            device_id=(sp, dp), device_id_type=MESH,
        ).start()

    def fetch(n, sem):
        pltpu.make_async_copy(up.at[0, :, lanes(n, c)], up_v.at[n], sem).start()
        pltpu.make_async_copy(cot.at[0, :, lanes(n, c)], cot_v.at[n], sem).start()

    def fetched(count, sem):
        drain(up_v.at[pl.ds(0, count)], sem)
        drain(cot_v.at[pl.ds(0, count)], sem)

    loop(quart, lambda k: fetch(order(k) * gd, in_one))

    barrier = pltpu.get_barrier_semaphore()

    def signal(sem, sp, dp):
        pl.semaphore_signal(sem, inc=1, device_id=(sp, dp), device_id_type=MESH)

    @pl.when(s < S - quart)
    def _():
        loop(mid, lambda k: signal(barrier, mid - mid * (s // mid) + k, d))

    loop(D - 1 - d, lambda k: signal(barrier, s, d + k + 1))
    loop(S - 1 - quart, lambda k: fetch(order(k + quart) * gd, in_ab.at[0]))
    fetch(s * gd, in_ab.at[0])
    loop(gd - 1, lambda g: loop(S, lambda j: fetch(j * gd + g + 1, in_ab.at[g + 1])))
    pl.semaphore_wait(barrier, jnp.where(low, quart, mid) + d)
    loop(d, lambda k: signal(dp_in, s, k))

    @pl.when(s >= S - quart)
    def _():
        loop(mid, lambda k: signal(last_in, k, d))

    @pl.when(s >= mid)
    def _():
        signal(near_in, s - mid, d)

    def send_weights(g):
        mine = w_full.at[g, sub(d, rows)]
        loop(half - 1, lambda k: remote(
            w.at[g], mine, sent.at[1], w_rx.at[g], s, lax.rem(d + 2 * k + 2, D)))
        remote(w.at[g], mine, sent.at[1], w_in.at[g], s, twin)

    def gate_chunk(n):
        x = up_v[n].astype(f32)
        a = (x * phi(x)).astype(bf16)
        return (cot_v[n].astype(f32) * a.astype(f32)).astype(bf16)

    def gate_send(g, k):
        peer = order(k)
        n = peer * gd + g
        gate_s[n] = gate_chunk(n)
        remote(gate_s.at[n], gate_h.at[g, my_rows, my_cols], sent.at[0], g_rcv.at[g], peer, d)

    def gate_far(g):
        fetched(S, in_ab.at[g])
        loop(mid, lambda k: gate_send(g, k))

    def gate_near(g):
        loop(mid - 1, lambda k: gate_send(g, k + mid))
        gate_h[g, my_rows, my_cols] = gate_chunk(s * gd + g)

    fetched(quart, in_one)
    loop(quart, lambda k: gate_send(0, k))

    @pl.when(low)
    def _():
        pl.semaphore_wait(last_in, quart)
        signal(near_in, s + mid, d)

    fetched(S - quart, in_ab.at[0])
    loop(mid - quart, lambda k: gate_send(0, k + quart))
    pltpu.make_async_copy(bias_in, bias, in_v).start()
    pltpu.make_async_copy(gain_in, gain, in_v).start()
    loop(groups, lambda n: pltpu.make_async_copy(val.at[0, :, lanes(n, c)], val_v.at[n], in_v).start())
    loop(gd - 1, lambda g: gate_far(g + 1))

    @pl.when(d < D - 1)
    def _():
        pl.semaphore_wait(dp_in, D - 1 - d)

    loop(gd, lambda g: pltpu.make_async_copy(w.at[g], w_full.at[g, sub(d, rows)], w_in.at[g]).start())
    loop(gd, send_weights)
    pl.semaphore_wait(near_in, 1)
    loop(gd, gate_near)

    drain(val_v, in_v)
    drain(bias, in_v)
    drain(gain, in_v)

    def stat(n, acc):
        x = val_v[n].astype(f32)
        a = x * phi(x)
        act[n] = a
        return acc + a * a

    total = lax.fori_loop(0, groups, stat, jnp.zeros((tok, c), f32))
    mean = jnp.sum(total, axis=1, keepdims=True) / width
    inv_b[...] = jnp.broadcast_to(lax.rsqrt(mean + norm_floor), (tok, c))

    def norm_group(g):
        def chunk(n):
            return (act[n] * inv_b[...] * gain[n]).astype(bf16)

        def one(k):
            peer = order(k)
            n = peer * gd + g
            norm_s[n] = chunk(n)
            remote(norm_s.at[n], norm_h.at[g, my_rows, my_cols], sent.at[0], v_rcv.at[g], peer, d)

        loop(S - 1, one)
        norm_h[g, my_rows, my_cols] = chunk(s * gd + g)

    loop(gd, norm_group)

    part = block * (S - 1) // S
    tile = min(block, 256)

    def give_back(g, src, dst, snd, rcv, near):
        def one(k):
            peer = late_order(k) if near else order(k)
            end = jnp.where((g == gd - 1) & inner & (k >= mid - 1), 1, 0) if near else 0
            remote(
                src.at[g, sub(lax.rem(peer, per_block), tok), lanes(peer // per_block, c)],
                dst.at[s * gd + g], snd, rcv.at[g + end] if near else rcv, peer, d)

        loop(S - 1, one)
        dst[s * gd + g] = src[g, my_rows, my_cols]

    def back_group(g):
        def forward(k):
            piece = w_full.at[g, sub(lax.rem(d + D - 2 * k - 2, D), rows)]
            remote(piece, piece, sent.at[1], w_in.at[g], s, twin)

        if half > 1:
            drain(w_full.at[g, pl.ds(0, (half - 1) * rows)], w_rx.at[g])
            loop(half - 1, forward)
        drain(w_full.at[g, pl.ds(0, (half + 1) * rows)], w_in.at[g])
        drain(gate_h.at[g, pl.ds(0, part)], g_rcv.at[g])

        def one(t):
            cols = lanes(t, tile)
            y = lax.dot_general(
                w_full[g, :, cols], gate_h[g], (((0,), (0,)), ((), ())), preferred_element_type=f32)
            back_s[g, sub(t, tile), :] = y.astype(bf16)

        loop(block // tile, one)
        give_back(g, back_s, back_t, sent.at[0], b_rcv, False)
        bias_s[g] = lax.dot_general(
            jnp.ones((8, blocks * c), bf16), gate_h[g], (((1,), (1,)), ((), ())),
            preferred_element_type=f32)

    loop(gd, back_group)
    loop(D - 1, lambda k: remote(
        bias_s.at[:, :, lanes(lax.rem(d + k + 1, D), rows)], bias_r.at[k], sent.at[3], bs_rcv,
        s, lax.rem(d + k + 1, D)))

    def mix_group(g):
        drain(norm_h.at[g, pl.ds(0, part)], v_rcv.at[g])
        n = s * gd + g

        def dot(t, acc):
            at = sub(t, 32)
            return acc + back_s[g, at, :].astype(f32) * norm_h[g, at, :].astype(f32)

        total = lax.fori_loop(0, block // 32, dot, jnp.zeros((32, blocks * c), f32))
        total = jnp.sum(total, axis=0, keepdims=True)
        total = sum(total[:, b * c:(b + 1) * c] for b in range(blocks))
        gain_d[g, d] = total / gain[n]
        loop(D - 1, lambda k: remote(
            gain_d.at[g, d], gain_d.at[g, d], sent.at[3], gx_rcv.at[g], s, lax.rem(d + k + 1, D)))

        def grad(peer):
            return lax.dot_general(
                gate_h[g, sub(peer, rows), :], norm_h[g], (((1,), (1,)), ((), ())),
                preferred_element_type=f32)

        def pair(k):
            wg_s[g, k] = grad(lax.rem(twin + 2 * k + 2, D)).astype(bf16)
            remote(wg_s.at[g, k], wg_t.at[g, k], sent.at[2], wt_rcv.at[g], s, twin)

        loop(half, pair)

        def mul(t):
            at = sub(t, tile)
            y = jnp.dot(w_full[g, at, :], norm_h[g], preferred_element_type=f32)
            col = jnp.broadcast_to(bias[pl.ds(g, 1), lanes(t, tile)], (c, tile)).T
            mix_s[g, at, :] = (y + jnp.concatenate([col] * blocks, axis=1)).astype(bf16)

        loop(block // tile, mul)
        drain(gain_d.at[g, pl.ds(0, D - 1)], gx_rcv.at[g])
        gain_all[n] = lax.fori_loop(
            0, D, lambda k, acc: acc + gain_d[g, k], jnp.zeros((1, c), f32))
        loop(S - 1, lambda k: remote(
            gain_all.at[n], gain_all.at[n], sent.at[3], gn_rcv, order(k), d))
        give_back(g, mix_s, mix_t, sent.at[0], m_rcv, True)
        drain(wg_t.at[g], wt_rcv.at[g])

        def across(k):
            peer = lax.rem(d + 2 * k + 2, D)
            wg_f[g, k] = (grad(peer) + wg_t[g, k].astype(f32)).astype(bf16)
            remote(wg_f.at[g, k], wg_r.at[g, k], sent.at[2], wg_rcv, s, peer)

        loop(half - 1, across)
        wg_o[g] = grad(d) + wg_t[g, half - 1].astype(f32)

    loop(gd, mix_group)

    drain(back_t.at[pl.ds(0, (S - 1) * gd)], b_rcv)

    def dots(n, acc):
        return acc + back_t[n].astype(f32) * act[n] * gain[n]

    total = lax.fori_loop(0, groups, dots, jnp.zeros((tok, c), f32))
    coef = jnp.sum(total, axis=1, keepdims=True) / width

    def value_out(n):
        inv = inv_b[...]
        scaled = back_t[n].astype(f32) * gain[n]
        y = inv * scaled - inv * inv * inv * act[n] * coef
        val_o[0, :, lanes(n, c)] = (y * slope(val_v[n].astype(f32))).astype(bf16)

    loop(groups, value_out)

    drain(bias_r, bs_rcv)
    total = lax.fori_loop(
        0, D - 1, lambda k, acc: acc + bias_r[k], bias_s[:, :, lanes(d, rows)])
    bg_o[...] = total[:, 0, :]

    def up_slope(n):
        act[n] = slope(up_v[n].astype(f32))

    loop(groups, up_slope)

    def sum_weight_grad(g):
        def one(t):
            at = sub(t, 32)
            acc = wg_o[g, at, :]
            for k in range(half - 1):
                acc = acc + wg_r[g, k, at, :].astype(f32)
            wg_o[g, at, :] = acc

        loop(rows // 32, one)

    if half > 1:
        drain(wg_r, wg_rcv)
    loop(gd, sum_weight_grad)

    def up_chunk(g, peer):
        n = peer * gd + g
        mid = (cot_v[n].astype(f32) * mix_t[n].astype(f32)).astype(bf16)
        up_o[0, :, lanes(n, c)] = (mid.astype(f32) * act[n]).astype(bf16)

    def up_group(g):
        drain(mix_t.at[pl.ds(0, S - 1)], m_rcv.at[g])
        loop(S, lambda peer: up_chunk(g, peer))

    inner_far = jnp.where(low, mid, quart)
    outer_far = jnp.where(low, mid + quart, 0)
    own = mid * (s // mid)
    loop(gd - 1, up_group)
    drain(mix_t.at[pl.ds(0, S - 1 - quart)], m_rcv.at[gd - 1])
    loop(mid, lambda k: up_chunk(gd - 1, own + k))
    loop(mid - quart, lambda k: up_chunk(gd - 1, outer_far + k))
    drain(mix_t.at[pl.ds(0, quart)], m_rcv.at[gd])
    loop(quart, lambda k: up_chunk(gd - 1, inner_far + k))
    chunks = pl.ds(0, (S - 1) * gd)
    drain(gain_all.at[chunks], gn_rcv)
    gg_o[...] = gain_all[...]

    drain(w_full.at[:, pl.ds(0, half * rows)], sent.at[1])
    if half > 1:
        drain(w_full.at[:, pl.ds(0, (half - 1) * rows)], sent.at[1])
    drain(gate_s.at[chunks], sent.at[0])
    drain(norm_s.at[chunks], sent.at[0])
    drain(back_t.at[chunks], sent.at[0])
    drain(mix_t.at[chunks], sent.at[0])
    drain(wg_s, sent.at[2])
    if half > 1:
        drain(wg_f, sent.at[2])
    drain(bias_r, sent.at[3])
    drain(gain_d.at[:, pl.ds(0, D - 1)], sent.at[3])
    drain(gain_all.at[chunks], sent.at[3])


def finish(*refs):
    ins, outs, sem = refs[:5], refs[5:10], refs[10]
    pairs = []
    for a, b in zip(ins, outs):
        parts = min(a.shape[-2], 128) // 32 if a.ndim == 3 else 1
        size = a.shape[-2] // max(parts, 1)
        for i in range(max(parts, 1)):
            at = (slice(None), pl.ds(i * size, size)) if parts > 1 else slice(None)
            pairs.append((a.at[at], b.at[at]))
    copies = [pltpu.make_async_copy(a, b, sem) for a, b in pairs]
    for copy in copies:
        copy.start()
    for copy in copies:
        copy.wait()


def shards(S, D, cotangent, up_pre, value_pre, spatial_weight, spatial_bias, value_gain):
    tok, width = cotangent.shape[1:]
    gd, rows, block = spatial_weight.shape
    groups = gd * S
    c = width // groups
    blocks = tok * S // block
    half = D // 2
    dma = pltpu.SemaphoreType.DMA
    vm = pltpu.VMEM
    tokens = vm((groups, tok, c), bf16)
    heads = vm((gd, block, blocks * c), bf16)
    scratch = [
        tokens, tokens, tokens, tokens, tokens, heads, heads,
        vm((gd, block, block), bf16), heads, heads, tokens, tokens,
        vm((gd, half, rows, block), bf16), vm((gd, half, rows, block), bf16),
        vm((gd, max(half - 1, 1), rows, block), bf16), vm((gd, max(half - 1, 1), rows, block), bf16),
        vm((groups, tok, c), f32), vm((tok, c), f32),
        vm((gd, 8, block), f32), vm((D - 1, gd, 8, rows), f32),
        vm((groups, 1, c), f32), vm((gd, D, 1, c), f32), vm((gd, block), f32), vm((groups, 1, c), f32),
        dma((gd,)), dma, dma((gd,)), dma((gd,)), dma((4,)), dma((gd,)), dma((gd,)), dma, dma((gd + 1,)),
        dma((gd,)), dma, dma, dma, dma((gd,)), pltpu.SemaphoreType.REGULAR, pltpu.SemaphoreType.REGULAR,
        pltpu.SemaphoreType.REGULAR, dma,
    ]
    anywhere = pl.BlockSpec(memory_space=pl.ANY)
    local = pl.BlockSpec(memory_space=pltpu.VMEM)
    outs = pl.pallas_call(
        functools.partial(kernel, S, D, gd, tok, block, blocks, c),
        out_shape=(
            vm((1, tok, width), bf16), vm((1, tok, width), bf16), vm((gd, rows, block), f32),
            vm((gd, rows), f32), vm((groups, 1, c), f32),
        ),
        in_specs=[anywhere] * 6,
        out_specs=(local,) * 5,
        scratch_shapes=scratch,
        compiler_params=pltpu.CompilerParams(
            collective_id=0, has_side_effects=True, vmem_limit_bytes=55 * 2**20),
    )(
        cotangent, up_pre, value_pre, spatial_weight,
        spatial_bias, value_gain.reshape(groups, 1, c),
    )
    outs = pl.pallas_call(
        finish,
        out_shape=[jax.ShapeDtypeStruct(o.shape, o.dtype) for o in outs],
        in_specs=[anywhere] * 5,
        out_specs=[anywhere] * 5,
        scratch_shapes=[dma],
        compiler_params=pltpu.CompilerParams(vmem_limit_bytes=2**20),
    )(*outs)
    return (*outs[:4], outs[4].reshape(width))


def solution(mesh):
    tokens = P("dp", "sp", None)
    return jax.shard_map(
        functools.partial(shards, mesh.shape["sp"], mesh.shape["dp"]),
        mesh=mesh,
        in_specs=(tokens, tokens, tokens, P("sp", "dp", None), P("sp", None), P()),
        out_specs=(tokens, tokens, P("sp", "dp", None), P("sp", "dp"), P()),
        check_vma=False,
    )
```
